32 devices in a mesh: rep: 2 (over x), fs: 8 (over z, y), tp: 2 (over core).
Axes of the slice: x: 2, y: 2, z: 4, core: 2. Of those that a mesh axis runs over, the one named last changes fastest.
Arguments:
- later_input: bfloat16 [2048, 2048], P(('rep', 'fs')), may hold values from -6 to 6
- earlier_input: bfloat16 [2048, 2048], P(('rep', 'fs')), may hold values from -6 to 6
- cotangent: bfloat16 [2048, 2048], P(('rep', 'fs')), may hold values from -6 to 6
- gate_weight: bfloat16 [2048, 3072], P('fs', 'tp'), may hold values from -0.125 to 0.125
- up_weight: bfloat16 [2048, 3072], P('fs', 'tp'), may hold values from -0.125 to 0.125
- down_weight: bfloat16 [2048, 3072], P('fs', 'tp'), may hold values from -0.109375 to 0.109375
- gate_sum: float32 [2048, 3072], P('fs', 'tp'), may hold values from -192 to 192
- up_sum: float32 [2048, 3072], P('fs', 'tp'), may hold values from -192 to 192
- down_sum: float32 [2048, 3072], P('fs', 'tp'), may hold values from -192 to 192
Outputs:
- later_output: bfloat16 [2048, 2048], P(('rep', 'fs'))
- earlier_input_grad: bfloat16 [2048, 2048], P(('rep', 'fs'))
- gate_sum_new: float32 [2048, 3072], P('fs', 'tp')
- up_sum_new: float32 [2048, 3072], P('fs', 'tp')
- down_sum_new: float32 [2048, 3072], P('fs', 'tp')
The draws below stay inside these ranges and needn't reach their ends.
All inputs are finite; a program needn't handle non-finite values.
Results may differ from the reference program's by a relative error of at most 0.02.
Values may be sent and summed in bfloat16 or wider, within the bound.
A program may use at most 128 MiB of HBM per device.

```python
import jax
import jax.numpy as jnp
from jax import lax

D = 2048
FF = 3072
TOKENS = 2048
N_TP = 2


def with_spikes(values, rng, source, target, blocks, factor):
    owner, partner = [(jnp.arange(values.shape[dim]) // (values.shape[dim] // blocks)).reshape([-1 if axis == dim else 1 for axis in range(values.ndim)]) for dim in (source, target)]
    chosen = jax.random.permutation(rng, blocks)[partner]
    strong = (owner == chosen) | (owner == (partner + blocks // 2) % blocks)
    return jnp.where(strong, factor * values, values)


def block_scale(key, extent, shards, smallest, largest):
    factor_of = 1.0
    for dim, parts in shards:
        heights = jax.random.uniform(jax.random.fold_in(jax.random.fold_in(key, 6), dim), (parts,), jnp.float32, smallest / len(shards), largest / len(shards))
        factor_of = factor_of * jnp.repeat(jnp.exp(heights), extent[dim] // parts).reshape((-1,) + (1,) * (len(extent) - 1 - dim))
    return factor_of


def normal_values(own_key, extent, scale, limit, pieces=(), kind=jnp.bfloat16):
    entries = scale * jax.random.normal(own_key, extent, jnp.float32)
    if pieces:
        entries = entries * block_scale(own_key, extent, pieces, -0.22, 0.18)
    return jnp.clip(entries, -limit, limit).astype(kind)


def bell_draw_with(rng, dims, scale, reach, split, heavy, held_as=jnp.bfloat16):
    values = scale * jax.random.normal(rng, dims, jnp.float32)
    if split:
        values = values * block_scale(rng, dims, split, -0.22, 0.18)
    return jnp.clip(with_spikes(values, jax.random.fold_in(rng, 3), *heavy), -reach, reach).astype(held_as)


def setup_inputs(seed: int = 0) -> dict:
    arg_keys = jax.random.split(jax.random.key(seed), 10)
    return {
        "later_input": normal_values(arg_keys[0], (TOKENS, D), 1.0, 6.0, ((0, 16),)),
        "earlier_input": normal_values(arg_keys[1], (TOKENS, D), 1.0, 6.0, ((0, 16),)),
        "cotangent": bell_draw_with(arg_keys[2], (TOKENS, D), 1.0, 6.0, ((0, 16),), (0, 1, 16, 2.0)),
        "gate_weight": normal_values(arg_keys[3], (D, FF), D ** -0.5, 0.125, ((0, 8), (1, 2))),
        "up_weight": normal_values(arg_keys[4], (D, FF), D ** -0.5, 0.125, ((0, 8), (1, 2))),
        "down_weight": normal_values(arg_keys[5], (D, FF), FF ** -0.5, 0.109375, ((0, 8), (1, 2))),
        "gate_sum": normal_values(arg_keys[6], (D, FF), 32.0, 192.0, ((0, 8), (1, 2)), jnp.float32),
        "up_sum": normal_values(arg_keys[7], (D, FF), 32.0, 192.0, ((0, 8), (1, 2)), jnp.float32),
        "down_sum": normal_values(arg_keys[8], (D, FF), 32.0, 192.0, ((0, 8), (1, 2)), jnp.float32),
    }


def contract_last(first, second):
    return lax.dot_general(first, second, (((1,), (1,)), ((), ())), preferred_element_type=jnp.float32)


def contract_first(first, second):
    return lax.dot_general(first, second, (((0,), (0,)), ((), ())), preferred_element_type=jnp.float32)


def blockwise(firsts, seconds):
    block_width = FF // N_TP
    running = jnp.zeros((firsts[0].shape[0], seconds[0].shape[0]), jnp.float32)
    for block_index in range(N_TP):
        lower = block_index * block_width
        partial_value = jnp.zeros_like(running)
        for first, second in zip(firsts, seconds):
            partial_value = partial_value + contract_last(first[:, lower:lower + block_width], second[:, lower:lower + block_width])
        rounded = lax.optimization_barrier(partial_value.astype(jnp.bfloat16))
        running = running + rounded.astype(jnp.float32)
    return running.astype(jnp.bfloat16)


def reference(later_input, earlier_input, cotangent, gate_weight, up_weight, down_weight, gate_sum, up_sum, down_sum):
    gate_late = jnp.dot(later_input, gate_weight, preferred_element_type=jnp.float32)
    up_late = jnp.dot(later_input, up_weight, preferred_element_type=jnp.float32)
    hidden_late = (jax.nn.silu(gate_late) * up_late).astype(jnp.bfloat16)
    later_output = blockwise([hidden_late], [down_weight])
    gate_early = jnp.dot(earlier_input, gate_weight, preferred_element_type=jnp.float32)
    up_early = jnp.dot(earlier_input, up_weight, preferred_element_type=jnp.float32)
    hidden_grad = jnp.dot(cotangent, down_weight, preferred_element_type=jnp.float32)
    sigmoid_gate = jax.nn.sigmoid(gate_early)
    silu_early = gate_early * sigmoid_gate
    gate_grad = (hidden_grad * up_early * sigmoid_gate * (1.0 + gate_early * (1.0 - sigmoid_gate))).astype(jnp.bfloat16)
    up_grad = (hidden_grad * silu_early).astype(jnp.bfloat16)
    hidden_early = (silu_early * up_early).astype(jnp.bfloat16)
    earlier_input_grad = blockwise([gate_grad, up_grad], [gate_weight, up_weight])
    gate_sum_new = gate_sum + contract_first(earlier_input, gate_grad)
    up_sum_new = up_sum + contract_first(earlier_input, up_grad)
    down_sum_new = down_sum + contract_first(cotangent, hidden_early)
    return later_output, earlier_input_grad, gate_sum_new, up_sum_new, down_sum_new
```

```python
import functools

import jax
import jax.numpy as jnp
from jax import lax
from jax.experimental import pallas as pl
from jax.experimental.pallas import tpu as pltpu
from jax.sharding import PartitionSpec as P

MESH = pl.DeviceIdType.MESH


def flip(index, k, n):
    out, bit = 0, 1
    while bit < n:
        digit = lax.rem(index // bit, 2)
        out = out + bit * ((1 - digit) if k & bit else digit)
        bit *= 2
    return out


def span(start, size, step):
    return pl.ds(pl.multiple_of(start, step), size)


def remote(source, target, send, recv, device):
    return pltpu.make_async_remote_copy(
        src_ref=source,
        dst_ref=target,
        send_sem=send,
        recv_sem=recv,
        device_id=device,
        device_id_type=MESH,
    )


def fused_kernel(
    nz, later, earlier, cot, gw, uw, dw, late_out, early_out, g_out,
    slots, w, hid, part, peer, rin, rout, fin, gown, gyo, gyi, gxo, gxi, gzo,
    wzs, wzr, wxs, wxr, wys, wyr, aos, ags, agr, cs, cr,
    tds, tdr, rss, rsr, os_, or_, gys, gyr, gxs, gxr, gzs, gzr, gfs, gfr,
):
    r, f, t = lax.axis_index("rep"), lax.axis_index("fs"), lax.axis_index("tp")
    y, z = lax.rem(f, 2), f // 2
    m, width = later.shape
    q = m // 2
    dl, u = gw.shape[0], w.shape[2]
    hr = dl // 2
    f32, bf16 = jnp.float32, jnp.bfloat16
    outs = (late_out, early_out)
    to_x, to_y, to_t = {"rep": 1 - r}, {"fs": z * 2 + 1 - y}, {"tp": 1 - t}

    def layer(height):
        return {"fs": height * 2 + y}

    barrier = pltpu.get_barrier_semaphore()
    for device in [layer(flip(z, k, nz)) for k in range(1, nz)] + [to_x, to_y, to_t]:
        pl.semaphore_signal(barrier, inc=1, device_id=device, device_id_type=MESH)
    pl.semaphore_wait(barrier, nz + 2)

    pending = []

    def go(copy):
        copy.start()
        pending.append((None, copy))

    def when_go(condition, copy):
        @pl.when(condition)
        def _():
            copy.start()

        pending.append((condition, copy))

    def rows(side, height, h):
        return span((height * 2 + side) * dl + h * hr, hr, hr)

    def piece(side, height, h):
        return w.at[:, rows(side, height, h), :]

    def units(height):
        return span(height * u, u, u)

    def send_inputs(height, send, recv, device):
        for i, weight in enumerate((gw, uw, dw)):
            remote(weight.at[span(r * hr, hr, hr), units(height)], w.at[i, rows(y, z, r), :], send, recv, device).start()
        block = piece(y, z, r)
        pending.append((None, remote(block, block, send, recv, device)))

    def wx(k, a, block):
        return remote(block, block, wxs.at[k, a], wxr.at[k, a], to_x)

    def wy(k, a, block):
        return remote(block, block, wys.at[k, a], wyr.at[k, a], to_y)

    def spread(k):
        block = piece(y, flip(z, k, nz), r)
        remote(block, block, wzs.at[k], wzr.at[k], to_x).wait_recv()
        go(wx(k, 0, block))
        go(wy(k, 0, block))

    def relay(k):
        height = flip(z, k, nz)
        if k % 2:
            block = piece(y, height, 1 - r)
            wx(k, 0, block).wait_recv()
            go(wy(k, 1, block))
        else:
            block = piece(1 - y, height, r)
            wy(k, 0, block).wait_recv()
            go(wx(k, 1, block))

    def gathered(k):
        height = flip(z, k, nz)
        if k % 2:
            wy(k, 0, piece(1 - y, height, r)).wait_recv()
            wy(k, 1, piece(1 - y, height, 1 - r)).wait_recv()
        else:
            if k:
                wx(k, 0, piece(y, height, 1 - r)).wait_recv()
            wx(k, 1, piece(1 - y, height, 1 - r)).wait_recv()

    arrays = (pl.ds(1, 2), pl.ds(0, 1))

    def half(core):
        return span(core * q, q, q)

    def block_of(g, origin, core):
        return slots.at[arrays[g], origin, half(core), :]

    def step_of(d):
        return 1 - 2 * d

    def exists(height):
        return jnp.logical_and(height >= 0, height < nz)

    def send_own(g):
        for d in range(2):
            device = layer(z + step_of(d))
            sources = ((1, earlier), (2, cot)) if g == 0 else ((0, later),)

            @pl.when(exists(z + step_of(d)))
            def _():
                for i, source in sources:
                    remote(
                        source.at[half(t), :], slots.at[i, z, half(t), :], aos.at[g, d], agr.at[g, z], device
                    ).start()

            block = block_of(g, z, t)
            pending.append((exists(z + step_of(d)), remote(block, block, aos.at[g, d], agr.at[g, z], device)))

    def take_on(g, k):
        for d in range(2):
            origin, target = z - step_of(d) * k, z + step_of(d)
            block = block_of(g, origin, t)
            ahead = remote(block, block, ags.at[g, k, d], agr.at[g, origin], layer(target))
            over = remote(block, block, cs.at[g, k, d], cr.at[g, k, d], to_t)

            @pl.when(exists(origin))
            def _():
                ahead.wait_recv()

            when_go(jnp.logical_and(exists(origin), exists(target)), ahead)
            when_go(exists(origin), over)

    def whole(g, k, d):
        block = block_of(g, z - step_of(d) * k, 1 - t)
        remote(block, block, cs.at[g, k, d], cr.at[g, k, d], to_t).wait_recv()

    def each_block(g, k, body):
        if k == 0:
            body(z)
            return
        for d in range(2):
            @pl.when(exists(z - step_of(d) * k))
            def _():
                whole(g, k, d)

        def one(d, carry):
            origin = z - step_of(d) * k

            @pl.when(exists(origin))
            def _():
                body(origin)

            return carry

        lax.fori_loop(0, 2, one, 0)

    def early(b):
        gate = jnp.dot(slots[1, b], w[0], preferred_element_type=f32)
        up = jnp.dot(slots[1, b], w[1], preferred_element_type=f32)
        hidden_grad = jnp.dot(slots[2, b], w[2], preferred_element_type=f32)
        hid[0, b], hid[1, b], hid[2, b] = early_parts(gate, up, hidden_grad)

    step = width // 4

    def trade(o, b):
        return remote(part.at[o, b, half(1 - t), :], peer.at[o, b], tds.at[o, b], tdr.at[o, b], to_t)

    def late(b):
        gate = jnp.dot(slots[0, b], w[0], preferred_element_type=f32)
        up = jnp.dot(slots[0, b], w[1], preferred_element_type=f32)
        hidden = (jax.nn.silu(gate) * up).astype(bf16)
        for c in range(4):
            lanes = slice(c * step, (c + 1) * step)
            part[0, b, :, lanes] = contract_last(hidden, w[2, lanes, :]).astype(bf16)
        trade(0, b).start()

    def input_grad(b, carry):
        for c in range(4):
            lanes = slice(c * step, (c + 1) * step)
            part[1, b, :, lanes] = (
                contract_last(hid[0, b], w[0, lanes, :]) + contract_last(hid[1, b], w[1, lanes, :])
            ).astype(bf16)
        trade(1, b).start()
        return carry

    def own(o, b):
        return part[o, b, half(t), :].astype(f32) + peer[o, b].astype(f32)

    def traded(o, b):
        remote(peer.at[o, b], peer.at[o, b], tds.at[o, b], tdr.at[o, b], to_t).wait_recv()

    def sum_copy(o, d, b):
        return remote(rout.at[o, b], rin.at[d, o, b], rss.at[o, b], rsr.at[d, o, b], layer(z + step_of(d)))

    def sum_pass(o, p):
        for d in range(2):
            @pl.when(z == (nz - 1 - p if d else p))
            def _():
                def one(i, carry):
                    b = i if d else nz - 1 - i
                    traded(o, b)
                    value = own(o, b)
                    if p:
                        slot = rin.at[d, o, b]
                        remote(slot, slot, rss.at[o, b], rsr.at[d, o, b], to_t).wait_recv()
                        value = value + rin[d, o, b].astype(f32)
                    rout[o, b] = value.astype(bf16)
                    sum_copy(o, d, b).start()
                    return carry

                lax.fori_loop(0, nz - 1 - p, one, 0)

    def sum_end(o):
        traded(o, z)
        fin[...] = own(o, z)
        for d in range(2):
            @pl.when(exists(z - step_of(d)))
            def _():
                slot = rin.at[d, o, z]
                remote(slot, slot, rss.at[o, z], rsr.at[d, o, z], to_t).wait_recv()
                fin[...] += rin[d, o, z].astype(f32)

        outs[o][half(t), :] = fin[...].astype(bf16)
        mine = outs[o].at[half(t), :]
        go(remote(mine, mine, os_.at[o], or_.at[o], to_t))

    def grad_block(side, height, i):
        lanes = span((height * 2 + side) * dl, dl, dl)
        source = slots[2 if i == 2 else 1, :, :, lanes].reshape(nz * m, dl)
        return contract_first(source, hid[i].reshape(nz * m, u))

    def grad_send(k):
        for i in range(3):
            gyo[k, i] = grad_block(1 - y, flip(z, k, nz), i).astype(bf16)
        go(remote(gyo.at[k], gyi.at[k], gys.at[k], gyr.at[k], to_y))

    def grad_own(k):
        for i in range(3):
            gown[k, i] = grad_block(y, flip(z, k, nz), i)

    def grad_x(k):
        remote(gyi.at[k], gyi.at[k], gys.at[k], gyr.at[k], to_y).wait_recv()
        theirs = span((1 - r) * hr, hr, hr)
        gxo[k] = (gown[k, :, theirs, :] + gyi[k, :, theirs, :].astype(f32)).astype(bf16)
        go(remote(gxo.at[k], gxi.at[k], gxs.at[k], gxr.at[k], to_x))

    def g_block(height, h):
        return g_out.at[:, span(h * hr, hr, hr), units(height)]

    def grad_z(k):
        remote(gxi.at[k], gxi.at[k], gxs.at[k], gxr.at[k], to_x).wait_recv()
        mine = span(r * hr, hr, hr)
        total = (
            gown[k, :, mine, :] + gyi[k, :, mine, :].astype(f32) + gxi[k].astype(f32)
        ).astype(bf16)
        if k:
            gzo[k] = total
            go(remote(gzo.at[k], g_block(z, r), gzs.at[k], gzr.at[k], layer(flip(z, k, nz))))
        else:
            g_out[:, mine, units(z)] = total

    def g_copy(k, h):
        block = g_block(flip(z, k, nz), h)
        return remote(block, block, gfs.at[k], gfr.at[k], to_x)

    def grad_x_back(k):
        if k:
            block = g_block(flip(z, k, nz), r)
            remote(block, block, gzs.at[k], gzr.at[k], to_x).wait_recv()
        go(g_copy(k, r))

    for k in range(1, nz):
        send_inputs(flip(z, k, nz), wzs.at[k], wzr.at[k], layer(flip(z, k, nz)))
    send_inputs(z, wys.at[0, 0], wyr.at[0, 0], to_y)
    send_own(0)
    slots[0, z] = later[...]
    slots[1, z] = earlier[...]
    slots[2, z] = cot[...]
    for i, weight in enumerate((gw, uw, dw)):
        w[i, span((z * 2 + y) * dl, dl, dl), :] = weight[:, units(z)]
    relay(0)
    for k in range(1, nz):
        spread(k)
        if k > 1:
            relay(k - 1)
    relay(nz - 1)
    take_on(0, 1)
    for k in range(nz):
        gathered(k)
    for k in range(nz):
        each_block(0, k, early)
        if k + 2 < nz:
            take_on(0, k + 2)
        if k == max(nz - 4, 0):
            send_own(1)
    take_on(1, 1)
    order = list(range(nz - 1, -1, -1))
    for k in order:
        grad_send(k)
    for k in range(2, nz):
        take_on(1, k)
    for k in order:
        grad_own(k)
    lax.fori_loop(0, nz, input_grad, 0)

    tasks = []
    for i in range(nz + 2):
        chain = []
        if i >= 2:
            chain.append((grad_x_back, order[i - 2]))
        if 1 <= i <= nz:
            chain.append((grad_z, order[i - 1]))
        if i < nz:
            chain.append((grad_x, order[i]))
        tasks.append(chain)
    for i in range(nz + 2):
        for task, k in tasks[i]:
            task(k)
        if i < nz:
            each_block(1, i, late)
        if i < nz - 1:
            sum_pass(1, i)
        if i == nz - 1:
            sum_end(1)
        if i >= 2 and i - 2 < nz - 1:
            pass
        if i == nz - 1:
            for p in range(nz - 1):
                sum_pass(0, p)
        if i == nz:
            sum_end(0)
    for k in range(nz):
        g_copy(k, 1 - r).wait_recv()
    for o in range(2):
        other = outs[o].at[half(1 - t), :]
        remote(other, other, os_.at[o], or_.at[o], to_t).wait_recv()
    for o in range(2):
        for b in range(nz):
            trade(o, b).wait_send()

            @pl.when(z != b)
            def _():
                sum_copy(o, 0, b).wait_send()

    for condition, copy in pending:
        if condition is None:
            copy.wait_send()
        else:
            @pl.when(condition)
            def _():
                copy.wait_send()


VMEM = pl.BlockSpec(memory_space=pltpu.VMEM)


def dma(*shape):
    return pltpu.SemaphoreType.DMA(shape)


def split_hidden(
    n,
    later_input,
    earlier_input,
    cotangent,
    gate_weight,
    up_weight,
    down_weight,
    gate_sum,
    up_sum,
    down_sum,
):
    bf16, f32 = jnp.bfloat16, jnp.float32
    m, width = later_input.shape
    dl, ff = gate_weight.shape
    nz = n // 2
    u, q, hr = ff // nz, m // 2, dl // 2
    later_output, earlier_input_grad, total = pl.pallas_call(
        functools.partial(fused_kernel, nz),
        out_shape=(
            jax.ShapeDtypeStruct((m, width), bf16),
            jax.ShapeDtypeStruct((m, width), bf16),
            jax.ShapeDtypeStruct((3, dl, ff), bf16),
        ),
        in_specs=[VMEM] * 6,
        out_specs=(VMEM, VMEM, VMEM),
        scratch_shapes=[
            pltpu.VMEM((3, nz, m, width), bf16),
            pltpu.VMEM((3, width, u), bf16),
            pltpu.VMEM((3, nz, m, u), bf16),
            pltpu.VMEM((2, nz, m, width), bf16),
            pltpu.VMEM((2, nz, q, width), bf16),
            pltpu.VMEM((2, 2, nz, q, width), bf16),
            pltpu.VMEM((2, nz, q, width), bf16),
            pltpu.VMEM((q, width), f32),
            pltpu.VMEM((nz, 3, dl, u), f32),
            pltpu.VMEM((nz, 3, dl, u), bf16),
            pltpu.VMEM((nz, 3, dl, u), bf16),
            pltpu.VMEM((nz, 3, hr, u), bf16),
            pltpu.VMEM((nz, 3, hr, u), bf16),
            pltpu.VMEM((nz, 3, hr, u), bf16),
        ]
        + [dma(nz)] * 2
        + [dma(nz, 2)] * 4
        + [dma(2, 2), dma(2, nz, 2), dma(2, nz), dma(2, nz, 2), dma(2, nz, 2)]
        + [dma(2, nz), dma(2, nz), dma(2, nz), dma(2, 2, nz), dma(2), dma(2)]
        + [dma(nz)] * 8,
        compiler_params=pltpu.CompilerParams(
            collective_id=0, has_side_effects=True, vmem_limit_bytes=50 * 2**20
        ),
        name="fused",
    )(later_input, earlier_input, cotangent, gate_weight, up_weight, down_weight)
    sums = tuple(old + total[i].astype(f32) for i, old in enumerate((gate_sum, up_sum, down_sum)))
    return (later_output, earlier_input_grad) + sums


def early_parts(gate_early, up_early, hidden_grad):
    sigmoid_gate = jax.nn.sigmoid(gate_early)
    silu_early = gate_early * sigmoid_gate
    gate_grad = (
        hidden_grad * up_early * sigmoid_gate * (1.0 + gate_early * (1.0 - sigmoid_gate))
    ).astype(jnp.bfloat16)
    up_grad = (hidden_grad * silu_early).astype(jnp.bfloat16)
    hidden_early = (silu_early * up_early).astype(jnp.bfloat16)
    return gate_grad, up_grad, hidden_early


def contract_last(first, second):
    return lax.dot_general(
        first, second, (((1,), (1,)), ((), ())), preferred_element_type=jnp.float32
    )


def contract_first(first, second):
    return lax.dot_general(
        first, second, (((0,), (0,)), ((), ())), preferred_element_type=jnp.float32
    )


def per_device(
    later_input,
    earlier_input,
    cotangent,
    gate_weight,
    up_weight,
    down_weight,
    gate_sum,
    up_sum,
    down_sum,
):
    gate_full, up_full, down_full = (
        lax.all_gather(gate_weight, "fs", axis=0, tiled=True),
        lax.all_gather(up_weight, "fs", axis=0, tiled=True),
        lax.all_gather(down_weight, "fs", axis=0, tiled=True),
    )
    gate_late = jnp.dot(later_input, gate_full, preferred_element_type=jnp.float32)
    up_late = jnp.dot(later_input, up_full, preferred_element_type=jnp.float32)
    hidden_late = (jax.nn.silu(gate_late) * up_late).astype(jnp.bfloat16)
    partial_late = contract_last(hidden_late, down_full)
    later_output = lax.psum(partial_late.astype(jnp.bfloat16), "tp")
    gate_early = jnp.dot(earlier_input, gate_full, preferred_element_type=jnp.float32)
    up_early = jnp.dot(earlier_input, up_full, preferred_element_type=jnp.float32)
    hidden_grad = jnp.dot(cotangent, down_full, preferred_element_type=jnp.float32)
    sigmoid_gate = jax.nn.sigmoid(gate_early)
    silu_early = gate_early * sigmoid_gate
    gate_grad = (
        hidden_grad * up_early * sigmoid_gate * (1.0 + gate_early * (1.0 - sigmoid_gate))
    ).astype(jnp.bfloat16)
    up_grad = (hidden_grad * silu_early).astype(jnp.bfloat16)
    hidden_early = (silu_early * up_early).astype(jnp.bfloat16)
    partial_early = contract_last(gate_grad, gate_full) + contract_last(up_grad, up_full)
    earlier_input_grad = lax.psum(partial_early.astype(jnp.bfloat16), "tp")
    columns, cot_columns = (
        lax.all_to_all(earlier_input, "fs", split_axis=1, concat_axis=0, tiled=True),
        lax.all_to_all(cotangent, "fs", split_axis=1, concat_axis=0, tiled=True),
    )
    gate_local = contract_first(columns, lax.all_gather(gate_grad, "fs", axis=0, tiled=True))
    up_local = contract_first(columns, lax.all_gather(up_grad, "fs", axis=0, tiled=True))
    down_local = contract_first(cot_columns, lax.all_gather(hidden_early, "fs", axis=0, tiled=True))
    gate_total, up_total, down_total = (
        lax.psum(gate_local.astype(jnp.bfloat16), "rep").astype(jnp.float32),
        lax.psum(up_local.astype(jnp.bfloat16), "rep").astype(jnp.float32),
        lax.psum(down_local.astype(jnp.bfloat16), "rep").astype(jnp.float32),
    )
    return (
        later_output,
        earlier_input_grad,
        gate_sum + gate_total,
        up_sum + up_total,
        down_sum + down_total,
    )


def solution(mesh):
    placed = (
        P(("rep", "fs"), None),
        P(("rep", "fs"), None),
        P(("rep", "fs"), None),
        P("fs", "tp"),
        P("fs", "tp"),
        P("fs", "tp"),
        P("fs", "tp"),
        P("fs", "tp"),
        P("fs", "tp"),
    )
    reps, shards, blocks = (mesh.shape[axis] for axis in ("rep", "fs", "tp"))

    def chosen(*arrays):
        rows = arrays[0].shape[0]
        depth, units = arrays[3].shape
        layers = shards // 2
        fits = (
            reps == 2
            and blocks == 2
            and layers >= 2
            and shards == 2 * layers
            and layers & (layers - 1) == 0
            and units % (layers * 128) == 0
            and depth % 128 == 0
            and rows % 32 == 0
            and arrays[0].shape[1] % 512 == 0
            and arrays[0].shape[1] == depth * shards
        )
        return split_hidden(shards, *arrays) if fits else per_device(*arrays)

    return jax.shard_map(
        chosen,
        mesh=mesh,
        in_specs=placed,
        out_specs=(
            P(("rep", "fs"), None),
            P(("rep", "fs"), None),
            P("fs", "tp"),
            P("fs", "tp"),
            P("fs", "tp"),
        ),
        check_vma=False,
    )
```

```python
import functools

import jax
import jax.numpy as jnp
from jax import lax
from jax.experimental import pallas as pl
from jax.experimental.pallas import tpu as pltpu
from jax.sharding import PartitionSpec as P

MESH = pl.DeviceIdType.MESH


def flip(index, k, n):
    out, bit = 0, 1
    while bit < n:
        digit = lax.rem(index // bit, 2)
        out = out + bit * ((1 - digit) if k & bit else digit)
        bit *= 2
    return out


def span(start, size, step):
    return pl.ds(pl.multiple_of(start, step), size)


def remote(source, target, send, recv, device):
    return pltpu.make_async_remote_copy(
        src_ref=source,
        dst_ref=target,
        send_sem=send,
        recv_sem=recv,
        device_id=device,
        device_id_type=MESH,
    )


EARLY, COT, LATE = 0, 1, 2


def fused_kernel(
    nz, later, earlier, cot, gw, uw, dw, gsum, usum, dsum, late_out, early_out, gnew, unew, dnew,
    slots, wt, w, g_out, hid, part, peer, rin, rout, gown, gyo, gyi, gxo, gxi, gzo,
    lts, lws, los, lns, wzs, wzr, wxs, wxr, wys, wyr, aos, ags, agr, cs, cr,
    tds, tdr, rss, rsr, os_, or_, gys, gyr, gxs, gxr, gzs, gzr, gfs, gfr,
):
    r, f, t = lax.axis_index("rep"), lax.axis_index("fs"), lax.axis_index("tp")
    y, z = lax.rem(f, 2), f // 2
    m, width = later.shape
    q = m // 2
    dl, u = gw.shape[0], w.shape[2]
    hr = dl // 2
    f32, bf16 = jnp.float32, jnp.bfloat16
    outs = (late_out, early_out)
    to_x, to_y, to_t = {"rep": 1 - r}, {"fs": z * 2 + 1 - y}, {"tp": 1 - t}

    def layer(height):
        return {"fs": height * 2 + y}

    def units(height):
        return span(height * u, u, u)

    slot_of = (1, 2, 0)
    local_tokens = [
        pltpu.make_async_copy(source, slots.at[slot_of[g], z], lts.at[g])
        for g, source in enumerate((earlier, cot, later))
    ]
    local_weights = [pltpu.make_async_copy(source, wt.at[i], lws.at[i]) for i, source in enumerate((gw, uw, dw))]
    local_own = [
        pltpu.make_async_copy(source.at[:, units(z)], w.at[i, span((z * 2 + y) * dl, dl, dl), :], los.at[i])
        for i, source in enumerate((gw, uw, dw))
    ]
    news = (gnew, unew, dnew)
    local_sums = [pltpu.make_async_copy(source, news[i], lns.at[i]) for i, source in enumerate((gsum, usum, dsum))]
    for copy in local_weights + local_tokens + local_own + local_sums:
        copy.start()

    barrier = pltpu.get_barrier_semaphore()
    for device in [layer(flip(z, k, nz)) for k in range(1, nz)] + [to_x, to_y, to_t]:
        pl.semaphore_signal(barrier, inc=1, device_id=device, device_id_type=MESH)
    pl.semaphore_wait(barrier, nz + 2)

    pending = []

    def go(copy):
        copy.start()
        pending.append((None, copy))

    def when_go(condition, copy):
        @pl.when(condition)
        def _():
            copy.start()

        pending.append((condition, copy))

    def rows(side, height, h):
        return span((height * 2 + side) * dl + h * hr, hr, hr)

    def piece(side, height, h):
        return w.at[:, rows(side, height, h), :]

    def send_weights(height, send, recv, device):
        go(remote(wt.at[:, span(r * hr, hr, hr), units(height)], piece(y, z, r), send, recv, device))

    def wx(k, a, block):
        return remote(block, block, wxs.at[k, a], wxr.at[k, a], to_x)

    def wy(k, a, block):
        return remote(block, block, wys.at[k, a], wyr.at[k, a], to_y)

    def spread(k):
        block = piece(y, flip(z, k, nz), r)
        remote(block, block, wzs.at[k], wzr.at[k], to_x).wait_recv()
        go(wx(k, 0, block))
        go(wy(k, 0, block))

    def relay(k):
        height = flip(z, k, nz)
        if k % 2:
            block = piece(y, height, 1 - r)
            wx(k, 0, block).wait_recv()
            go(wy(k, 1, block))
        else:
            block = piece(1 - y, height, r)
            wy(k, 0, block).wait_recv()
            go(wx(k, 1, block))

    def gathered(k):
        height = flip(z, k, nz)
        if k % 2:
            wy(k, 0, piece(1 - y, height, r)).wait_recv()
            wy(k, 1, piece(1 - y, height, 1 - r)).wait_recv()
        else:
            if k:
                wx(k, 0, piece(y, height, 1 - r)).wait_recv()
            wx(k, 1, piece(1 - y, height, 1 - r)).wait_recv()

    def half(core):
        return span(core * q, q, q)

    def block_of(g, origin, core):
        return slots.at[slot_of[g], origin, half(core), :]

    def step_of(d):
        return 1 - 2 * d

    def exists(height):
        return jnp.logical_and(height >= 0, height < nz)

    def send_own(g):
        for d in range(2):
            target = z + step_of(d)
            block = block_of(g, z, t)
            when_go(exists(target), remote(block, block, aos.at[g, d], agr.at[g, z], layer(target)))

    def take_on(g, k):
        for d in range(2):
            origin, target = z - step_of(d) * k, z + step_of(d)
            block = block_of(g, origin, t)
            ahead = remote(block, block, ags.at[g, k, d], agr.at[g, origin], layer(target))
            over = remote(block, block, cs.at[g, k, d], cr.at[g, k, d], to_t)

            @pl.when(exists(origin))
            def _():
                ahead.wait_recv()

            when_go(jnp.logical_and(exists(origin), exists(target)), ahead)
            when_go(exists(origin), over)

    def whole(g, k):
        for d in range(2):
            block = block_of(g, z - step_of(d) * k, 1 - t)

            @pl.when(exists(z - step_of(d) * k))
            def _():
                remote(block, block, cs.at[g, k, d], cr.at[g, k, d], to_t).wait_recv()

    def each_block(k, body):
        if k == 0:
            body(z)
            return

        def one(d, carry):
            origin = z - (1 - 2 * d) * k

            @pl.when(exists(origin))
            def _():
                body(origin)

            return carry

        lax.fori_loop(0, 2, one, 0)

    def early(b):
        gate = jnp.dot(slots[1, b], w[0], preferred_element_type=f32)
        up = jnp.dot(slots[1, b], w[1], preferred_element_type=f32)
        hidden_grad = jnp.dot(slots[2, b], w[2], preferred_element_type=f32)
        hid[0, b], hid[1, b], hid[2, b] = early_parts(gate, up, hidden_grad)

    def early_level(k):
        if k:
            whole(EARLY, k)
            whole(COT, k)
        each_block(k, early)

    step = width // 4

    def trade(o, b):
        return remote(part.at[o, b, half(1 - t), :], peer.at[o, b], tds.at[o, b], tdr.at[o, b], to_t)

    def late(b):
        gate = jnp.dot(slots[0, b], w[0], preferred_element_type=f32)
        up = jnp.dot(slots[0, b], w[1], preferred_element_type=f32)
        hidden = (jax.nn.silu(gate) * up).astype(bf16)
        for c in range(4):
            lanes = slice(c * step, (c + 1) * step)
            part[0, b, :, lanes] = contract_last(hidden, w[2, lanes, :]).astype(bf16)
        trade(0, b).start()

    def late_level(k):
        if k:
            whole(LATE, k)
        each_block(k, late)

    def input_grad(b):
        for c in range(4):
            lanes = slice(c * step, (c + 1) * step)
            part[1, b, :, lanes] = (
                contract_last(hid[0, b], w[0, lanes, :]) + contract_last(hid[1, b], w[1, lanes, :])
            ).astype(bf16)
        trade(1, b).start()

    fine = 16

    def traded(o, b):
        remote(peer.at[o, b], peer.at[o, b], tds.at[o, b], tdr.at[o, b], to_t).wait_recv()

    def chunks(body):
        def one(i, carry):
            body(i * fine)
            return carry

        lax.fori_loop(0, q // fine, one, 0)

    def own(o, b, start):
        return (
            part[o, b, span(t * q + start, fine, fine), :].astype(f32)
            + peer[o, b, span(start, fine, fine), :].astype(f32)
        )

    def sum_copy(o, d, b, device):
        return remote(rout.at[o, b], rin.at[d, o, b], rss.at[o, b], rsr.at[d, o, b], device)

    def sum_step(o, far, h):
        @pl.when(jnp.logical_or(z == h, z == nz - 1 - h))
        def _():
            up = jnp.where(z == h, 1, 0)
            d = 1 - up
            b = up * far + d * (nz - 1 - far)
            copy = sum_copy(o, d, b, layer(z + 2 * up - 1))
            traded(o, b)
            if h:
                copy.wait_recv()

            def add(start):
                piece_rows = span(start, fine, fine)
                value = own(o, b, start)
                if h:
                    value = value + rin[d, o, b, piece_rows, :].astype(f32)
                rout[o, b, piece_rows, :] = value.astype(bf16)

            chunks(add)
            copy.start()

    def sum_end(o):
        traded(o, z)
        for d in range(2):
            @pl.when(exists(z - step_of(d)))
            def _():
                sum_copy(o, d, z, to_t).wait_recv()

        def add(start):
            piece_rows = span(start, fine, fine)
            value = own(o, z, start)
            for d in range(2):
                value = value + jnp.where(
                    exists(z - step_of(d)), rin[d, o, z, piece_rows, :].astype(f32), 0.0
                )
            outs[o][span(t * q + start, fine, fine), :] = value.astype(bf16)

        chunks(add)
        mine = outs[o].at[half(t), :]
        go(remote(mine, mine, os_.at[o], or_.at[o], to_t))

    def grad_block(side, height, i):
        lanes = span((height * 2 + side) * dl, dl, dl)
        source = slots[2 if i == 2 else 1, :, :, lanes].reshape(nz * m, dl)
        return contract_first(source, hid[i].reshape(nz * m, u))

    def grad_send(k, i):
        gyo[k, i] = grad_block(1 - y, flip(z, k, nz), i).astype(bf16)
        go(remote(gyo.at[k, i], gyi.at[k, i], gys.at[k, i], gyr.at[k, i], to_y))

    def grad_own(k, i):
        gown[k, i] = grad_block(y, flip(z, k, nz), i)

    mine_rows, their_rows = span(r * hr, hr, hr), span((1 - r) * hr, hr, hr)

    def grad_x(k, i):
        remote(gyi.at[k, i], gyi.at[k, i], gys.at[k, i], gyr.at[k, i], to_y).wait_recv()
        gxo[k, i] = (gown[k, i, their_rows, :] + gyi[k, i, their_rows, :].astype(f32)).astype(bf16)
        go(remote(gxo.at[k, i], gxi.at[k, i], gxs.at[k, i], gxr.at[k, i], to_x))

    def g_block(i, height, h):
        return g_out.at[i, span(h * hr, hr, hr), units(height)]

    def grad_z(k, i):
        remote(gxi.at[k, i], gxi.at[k, i], gxs.at[k, i], gxr.at[k, i], to_x).wait_recv()
        total = (
            gown[k, i, mine_rows, :] + gyi[k, i, mine_rows, :].astype(f32) + gxi[k, i].astype(f32)
        ).astype(bf16)
        if k:
            gzo[k, i] = total
            go(remote(gzo.at[k, i], g_block(i, z, r), gzs.at[k, i], gzr.at[k, i], layer(flip(z, k, nz))))
        else:
            g_out[i, mine_rows, units(z)] = total

    def g_copy(k, i, h):
        block = g_block(i, flip(z, k, nz), h)
        return remote(block, block, gfs.at[k, i], gfr.at[k, i], to_x)

    def grad_back(k, i):
        if k:
            block = g_block(i, flip(z, k, nz), r)
            remote(block, block, gzs.at[k, i], gzr.at[k, i], to_x).wait_recv()
        go(g_copy(k, i, r))
        grad_add(k, i, r)

    def grad_add(k, i, h):
        place = (span(h * hr, hr, hr), units(flip(z, k, nz)))
        news[i][place] += g_out[(i,) + place].astype(f32)

    def grad_last(k, i):
        g_copy(k, i, 1 - r).wait_recv()
        grad_add(k, i, 1 - r)

    def run(name, task, *args):
        with jax.named_scope(name + "_".join(str(a) for a in args if isinstance(a, int))):
            task(*args)

    def send_first():
        for copy in local_weights:
            copy.wait()
        for k in range(1, nz):
            send_weights(flip(z, k, nz), wzs.at[k], wzr.at[k], layer(flip(z, k, nz)))
        send_weights(z, wys.at[0, 0], wyr.at[0, 0], to_y)
        for copy in local_tokens:
            copy.wait()
        send_own(EARLY)
        send_own(COT)
        for copy in local_own:
            copy.wait()

    last = nz - 1
    run("send_first", send_first)
    run("relay", relay, 0)
    for k in range(1, nz):
        run("spread", spread, k)
        if k > 1:
            run("relay", relay, k - 1)
    run("take_e", take_on, EARLY, 1)
    run("relay", relay, last)
    run("take_c", take_on, COT, 1)
    for k in range(last):
        run("gathered", gathered, k)
    if last > 1:
        run("take_e", take_on, EARLY, 2)
    run("gathered", gathered, last)
    run("early", early_level, 0)
    if last > 1:
        run("take_c", take_on, COT, 2)
    for k in range(3, last):
        run("take_e", take_on, EARLY, k)
        run("take_c", take_on, COT, k)
    run("send_l", send_own, LATE)
    run("early", early_level, 1)
    if last > 1:
        run("input_grad", each_block, 0, input_grad)
        run("input_grad", each_block, 1, input_grad)
    for k in range(2, last):
        run("early", early_level, k)
        run("sum_e", sum_step, 1, k - 1, 0)
        run("input_grad", each_block, k, input_grad)
    if last > 2:
        run("sum_e", sum_step, 1, last - 1, 0)
        run("take_e", take_on, EARLY, last)
        run("take_c", take_on, COT, last)
    if last > 1:
        run("early", early_level, last)
    order = [(k, i) for k in range(last, -1, -1) for i in range(3)]
    def send_next(count):
        for _ in range(count):
            if to_send:
                run("grad_send", grad_send, *to_send.pop(0))

    def own_next(count):
        for _ in range(count):
            if to_own:
                run("grad_own", grad_own, *to_own.pop(0))

    to_send, to_own = list(order), list(order)
    send_next(4)
    run("take_l", take_on, LATE, 1)
    for copy in local_sums:
        copy.wait()
    if last == 1:
        run("input_grad", each_block, 0, input_grad)
    if last == 2:
        run("sum_e", sum_step, 1, 1, 0)
    run("input_grad", each_block, last, input_grad)
    send_next(1)
    own_next(2)
    run("sum_e", sum_step, 1, last, 0)
    send_next(1)
    run("late", late_level, 0)
    run("late", late_level, 1)

    between = {}

    def place(j, *task):
        between.setdefault(j, []).append(task)

    for far in range(2, nz):
        place(3 * (far - 2), "take_l", take_on, LATE, far)
        place(3 * (far - 2) + 1, "late", late_level, far)
        for h in range(1, far):
            place(2 * (far - 2) - 1 + 4 * (h - 1), "sum_e", sum_step, 1, far, h)
            place(2 * (far - 2) + 7 + 3 * (h - 1), "sum_l", sum_step, 0, far, h)
    for far in range(1, nz):
        place(far + 2, "sum_l", sum_step, 0, far, 0)
    place(6 * last - 10, "sum_end_e", sum_end, 1)
    place(5 * last, "sum_end_l", sum_end, 0)
    count, lag = len(order), 5
    for j in range(min(min(between), -1), max(max(between), count + lag - 1) + 1):
        if 0 <= j < count:
            own_next(1)
            run("grad_x", grad_x, *order[j])
            send_next(1)
        if 1 <= j <= count:
            run("grad_z", grad_z, *order[j - 1])
            if order[j - 1][0] == 0:
                run("grad_back", grad_back, *order[j - 1])
        if lag <= j < count + lag and order[j - lag][0]:
            run("grad_back", grad_back, *order[j - lag])
        for name, task, *args in between.get(j, ()):
            run(name, task, *args)
    for k, i in order:
        run("grad_last", grad_last, k, i)
    for o in range(2):
        other = outs[o].at[half(1 - t), :]
        remote(other, other, os_.at[o], or_.at[o], to_t).wait_recv()
    for o in range(2):
        for b in range(nz):
            trade(o, b).wait_send()

            @pl.when(z != b)
            def _():
                sum_copy(o, 0, b, to_t).wait_send()

    for condition, copy in pending:
        if condition is None:
            copy.wait_send()
        else:
            @pl.when(condition)
            def _():
                copy.wait_send()


def close_kernel(*refs):
    sems = refs[-1]
    count = (len(refs) - 1) // 2
    copies = [pltpu.make_async_copy(refs[i], refs[count + i], sems.at[i]) for i in range(count)]
    for copy in copies:
        copy.start()
    for copy in copies:
        copy.wait()


def close(*arrays):
    return pl.pallas_call(
        close_kernel,
        out_shape=tuple(jax.ShapeDtypeStruct(a.shape, a.dtype) for a in arrays),
        in_specs=[VMEM] * len(arrays),
        out_specs=(HBM,) * len(arrays),
        scratch_shapes=[dma(len(arrays))],
        compiler_params=pltpu.CompilerParams(vmem_limit_bytes=8 * 2**20),
        name="close",
    )(*arrays)


VMEM = pl.BlockSpec(memory_space=pltpu.VMEM)
HBM = pl.BlockSpec(memory_space=pltpu.HBM)


def dma(*shape):
    return pltpu.SemaphoreType.DMA(shape)


def split_hidden(
    n,
    later_input,
    earlier_input,
    cotangent,
    gate_weight,
    up_weight,
    down_weight,
    gate_sum,
    up_sum,
    down_sum,
):
    bf16, f32 = jnp.bfloat16, jnp.float32
    m, width = later_input.shape
    dl, ff = gate_weight.shape
    nz = n // 2
    u, q, hr = ff // nz, m // 2, dl // 2
    results = pl.pallas_call(
        functools.partial(fused_kernel, nz),
        out_shape=(
            jax.ShapeDtypeStruct((m, width), bf16),
            jax.ShapeDtypeStruct((m, width), bf16),
            jax.ShapeDtypeStruct((dl, ff), f32),
            jax.ShapeDtypeStruct((dl, ff), f32),
            jax.ShapeDtypeStruct((dl, ff), f32),
        ),
        in_specs=[HBM] * 9,
        out_specs=(VMEM,) * 5,
        scratch_shapes=[
            pltpu.VMEM((3, nz, m, width), bf16),
            pltpu.VMEM((3, dl, ff), bf16),
            pltpu.VMEM((3, width, u), bf16),
            pltpu.VMEM((3, dl, ff), bf16),
            pltpu.VMEM((3, nz, m, u), bf16),
            pltpu.VMEM((2, nz, m, width), bf16),
            pltpu.VMEM((2, nz, q, width), bf16),
            pltpu.VMEM((2, 2, nz, q, width), bf16),
            pltpu.VMEM((2, nz, q, width), bf16),
            pltpu.VMEM((nz, 3, dl, u), f32),
            pltpu.VMEM((nz, 3, dl, u), bf16),
            pltpu.VMEM((nz, 3, dl, u), bf16),
            pltpu.VMEM((nz, 3, hr, u), bf16),
            pltpu.VMEM((nz, 3, hr, u), bf16),
            pltpu.VMEM((nz, 3, hr, u), bf16),
        ]
        + [dma(3)] * 4
        + [dma(nz)] * 2
        + [dma(nz, 2)] * 4
        + [dma(3, 2), dma(3, nz, 2), dma(3, nz), dma(3, nz, 2), dma(3, nz, 2)]
        + [dma(2, nz), dma(2, nz), dma(2, nz), dma(2, 2, nz), dma(2), dma(2)]
        + [dma(nz, 3)] * 8,
        compiler_params=pltpu.CompilerParams(
            collective_id=0, has_side_effects=True, vmem_limit_bytes=44 * 2**20
        ),
        name="fused",
    )(
        *(
            pltpu.with_memory_space_constraint(a, pltpu.HBM)
            for a in (later_input, earlier_input, cotangent, gate_weight, up_weight, down_weight, gate_sum, up_sum, down_sum)
        )
    )
    return close(*results)


def early_parts(gate_early, up_early, hidden_grad):
    sigmoid_gate = jax.nn.sigmoid(gate_early)
    silu_early = gate_early * sigmoid_gate
    gate_grad = (
        hidden_grad * up_early * sigmoid_gate * (1.0 + gate_early * (1.0 - sigmoid_gate))
    ).astype(jnp.bfloat16)
    up_grad = (hidden_grad * silu_early).astype(jnp.bfloat16)
    hidden_early = (silu_early * up_early).astype(jnp.bfloat16)
    return gate_grad, up_grad, hidden_early


def contract_last(first, second):
    return lax.dot_general(
        first, second, (((1,), (1,)), ((), ())), preferred_element_type=jnp.float32
    )


def contract_first(first, second):
    return lax.dot_general(
        first, second, (((0,), (0,)), ((), ())), preferred_element_type=jnp.float32
    )


def per_device(
    later_input,
    earlier_input,
    cotangent,
    gate_weight,
    up_weight,
    down_weight,
    gate_sum,
    up_sum,
    down_sum,
):
    gate_full, up_full, down_full = (
        lax.all_gather(gate_weight, "fs", axis=0, tiled=True),
        lax.all_gather(up_weight, "fs", axis=0, tiled=True),
        lax.all_gather(down_weight, "fs", axis=0, tiled=True),
    )
    gate_late = jnp.dot(later_input, gate_full, preferred_element_type=jnp.float32)
    up_late = jnp.dot(later_input, up_full, preferred_element_type=jnp.float32)
    hidden_late = (jax.nn.silu(gate_late) * up_late).astype(jnp.bfloat16)
    partial_late = contract_last(hidden_late, down_full)
    later_output = lax.psum(partial_late.astype(jnp.bfloat16), "tp")
    gate_early = jnp.dot(earlier_input, gate_full, preferred_element_type=jnp.float32)
    up_early = jnp.dot(earlier_input, up_full, preferred_element_type=jnp.float32)
    hidden_grad = jnp.dot(cotangent, down_full, preferred_element_type=jnp.float32)
    sigmoid_gate = jax.nn.sigmoid(gate_early)
    silu_early = gate_early * sigmoid_gate
    gate_grad = (
        hidden_grad * up_early * sigmoid_gate * (1.0 + gate_early * (1.0 - sigmoid_gate))
    ).astype(jnp.bfloat16)
    up_grad = (hidden_grad * silu_early).astype(jnp.bfloat16)
    hidden_early = (silu_early * up_early).astype(jnp.bfloat16)
    partial_early = contract_last(gate_grad, gate_full) + contract_last(up_grad, up_full)
    earlier_input_grad = lax.psum(partial_early.astype(jnp.bfloat16), "tp")
    columns, cot_columns = (
        lax.all_to_all(earlier_input, "fs", split_axis=1, concat_axis=0, tiled=True),
        lax.all_to_all(cotangent, "fs", split_axis=1, concat_axis=0, tiled=True),
    )
    gate_local = contract_first(columns, lax.all_gather(gate_grad, "fs", axis=0, tiled=True))
    up_local = contract_first(columns, lax.all_gather(up_grad, "fs", axis=0, tiled=True))
    down_local = contract_first(cot_columns, lax.all_gather(hidden_early, "fs", axis=0, tiled=True))
    gate_total, up_total, down_total = (
        lax.psum(gate_local.astype(jnp.bfloat16), "rep").astype(jnp.float32),
        lax.psum(up_local.astype(jnp.bfloat16), "rep").astype(jnp.float32),
        lax.psum(down_local.astype(jnp.bfloat16), "rep").astype(jnp.float32),
    )
    return (
        later_output,
        earlier_input_grad,
        gate_sum + gate_total,
        up_sum + up_total,
        down_sum + down_total,
    )


def solution(mesh):
    placed = (
        P(("rep", "fs"), None),
        P(("rep", "fs"), None),
        P(("rep", "fs"), None),
        P("fs", "tp"),
        P("fs", "tp"),
        P("fs", "tp"),
        P("fs", "tp"),
        P("fs", "tp"),
        P("fs", "tp"),
    )
    reps, shards, blocks = (mesh.shape[axis] for axis in ("rep", "fs", "tp"))

    def chosen(*arrays):
        rows = arrays[0].shape[0]
        depth, units = arrays[3].shape
        layers = shards // 2
        fits = (
            reps == 2
            and blocks == 2
            and layers >= 2
            and shards == 2 * layers
            and layers & (layers - 1) == 0
            and units % (layers * 128) == 0
            and depth % 128 == 0
            and rows % 64 == 0
            and arrays[0].shape[1] % 512 == 0
            and arrays[0].shape[1] == depth * shards
        )
        return split_hidden(shards, *arrays) if fits else per_device(*arrays)

    return jax.shard_map(
        chosen,
        mesh=mesh,
        in_specs=placed,
        out_specs=(
            P(("rep", "fs"), None),
            P(("rep", "fs"), None),
            P("fs", "tp"),
            P("fs", "tp"),
            P("fs", "tp"),
        ),
        check_vma=False,
    )
```

```python
import functools

import jax
import jax.numpy as jnp
from jax import lax
from jax.experimental import pallas as pl
from jax.experimental.pallas import tpu as pltpu
from jax.sharding import PartitionSpec as P

MESH = pl.DeviceIdType.MESH


def flip(index, k, n):
    out, bit = 0, 1
    while bit < n:
        digit = lax.rem(index // bit, 2)
        out = out + bit * ((1 - digit) if k & bit else digit)
        bit *= 2
    return out


def span(start, size, step):
    return pl.ds(pl.multiple_of(start, step), size)


def remote(source, target, send, recv, device):
    return pltpu.make_async_remote_copy(
        src_ref=source,
        dst_ref=target,
        send_sem=send,
        recv_sem=recv,
        device_id=device,
        device_id_type=MESH,
    )


EARLY, COT, LATE = 0, 1, 2


def fused_kernel(
    nz, later, earlier, cot, gw, uw, dw, gsum, usum, dsum, late_out, early_out, gnew, unew, dnew,
    slots, wt, w, g_out, hid, part, peer, rin, rout, gown, gboth, gyo, gyi, gxo, gxi, gzo,
    lts, lws, los, lns, wzs, wzr, wxs, wxr, wys, wyr, aos, ags, agr, cs, cr,
    tds, tdr, rss, rsr, os_, or_, gys, gyr, gxs, gxr, gzs, gzr, gfs, gfr,
):
    r, f, t = lax.axis_index("rep"), lax.axis_index("fs"), lax.axis_index("tp")
    y, z = lax.rem(f, 2), f // 2
    m, width = later.shape
    q = m // 2
    dl, u = gw.shape[0], w.shape[2]
    hr, last = dl // 2, nz - 1
    f32, bf16 = jnp.float32, jnp.bfloat16
    outs = (late_out, early_out)
    to_x, to_y, to_t = {"rep": 1 - r}, {"fs": z * 2 + 1 - y}, {"tp": 1 - t}

    def layer(height):
        return {"fs": height * 2 + y}

    def units(height):
        return span(height * u, u, u)

    slot_of = (1, 2, 0)
    local_tokens = [
        pltpu.make_async_copy(source, slots.at[slot_of[g], z], lts.at[g])
        for g, source in enumerate((earlier, cot, later))
    ]
    local_weights = [pltpu.make_async_copy(source, wt.at[i], lws.at[i]) for i, source in enumerate((gw, uw, dw))]
    local_own = [
        pltpu.make_async_copy(source.at[:, units(z)], w.at[i, span((z * 2 + y) * dl, dl, dl), :], los.at[i])
        for i, source in enumerate((gw, uw, dw))
    ]
    news = (gnew, unew, dnew)
    local_sums = [pltpu.make_async_copy(source, news[i], lns.at[i]) for i, source in enumerate((gsum, usum, dsum))]
    for copy in local_weights + local_tokens + local_own + local_sums:
        copy.start()

    barrier = pltpu.get_barrier_semaphore()
    for device in [layer(flip(z, k, nz)) for k in range(1, nz)] + [to_x, to_y, to_t]:
        pl.semaphore_signal(barrier, inc=1, device_id=device, device_id_type=MESH)
    pl.semaphore_wait(barrier, nz + 2)

    pending = []

    def go(copy):
        copy.start()
        pending.append((None, copy))

    def when_go(condition, copy):
        @pl.when(condition)
        def _():
            copy.start()

        pending.append((condition, copy))

    def rows(side, height, h):
        return span((height * 2 + side) * dl + h * hr, hr, hr)

    def piece(side, height, h):
        return w.at[:, rows(side, height, h), :]

    def send_weights(height, send, recv, device):
        remote(wt.at[:, span(r * hr, hr, hr), units(height)], piece(y, z, r), send, recv, device).start()

    def wx(k, a, block):
        return remote(block, block, wxs.at[0], wxr.at[k, a], to_x)

    def wy(k, a, block):
        return remote(block, block, wys.at[0], wyr.at[k, a], to_y)

    def spread(k):
        block = piece(y, flip(z, k, nz), r)
        remote(block, block, wzs.at[0], wzr.at[k], to_x).wait_recv()
        wx(k, 0, block).start()
        wy(k, 0, block).start()

    def relay(k):
        height = flip(z, k, nz)
        if k % 2:
            block = piece(y, height, 1 - r)
            wx(k, 0, block).wait_recv()
            wy(k, 1, block).start()
        else:
            block = piece(1 - y, height, r)
            wy(k, 0, block).wait_recv()
            wx(k, 1, block).start()

    def gathered(k):
        height = flip(z, k, nz)
        if k % 2:
            wy(k, 0, piece(1 - y, height, r)).wait_recv()
            wy(k, 1, piece(1 - y, height, 1 - r)).wait_recv()
        else:
            if k:
                wx(k, 0, piece(y, height, 1 - r)).wait_recv()
            wx(k, 1, piece(1 - y, height, 1 - r)).wait_recv()

    def half(core):
        return span(core * q, q, q)

    def block_of(g, origin, core):
        return slots.at[slot_of[g], origin, half(core), :]

    def step_of(d):
        return 1 - 2 * d

    def exists(height):
        return jnp.logical_and(height >= 0, height < nz)

    def send_own(g, ends=None):
        for d in range(2):
            target = z + step_of(d)
            block = block_of(g, z, t)
            at_end = z == (last if d else 0)
            chosen = exists(target)
            if ends is not None:
                chosen = jnp.logical_and(chosen, at_end if ends else jnp.logical_not(at_end))
            when_go(chosen, remote(block, block, aos.at[g, d], agr.at[g, z], layer(target)))

    def take_on(g, k):
        for d in range(2):
            origin, target = z - step_of(d) * k, z + step_of(d)
            block = block_of(g, origin, t)
            ahead = remote(block, block, ags.at[g, min(k, last - 1), d], agr.at[g, origin], layer(target))

            @pl.when(exists(origin))
            def _():
                ahead.wait_recv()

            if k < last:
                when_go(jnp.logical_and(exists(origin), exists(target)), ahead)

            @pl.when(exists(origin))
            def _():
                remote(block, block, cs.at[0], cr.at[g, origin], to_t).start()

    def whole(g, k):
        for d in range(2):
            origin = z - step_of(d) * k
            block = block_of(g, origin, 1 - t)

            @pl.when(exists(origin))
            def _():
                remote(block, block, cs.at[0], cr.at[g, origin], to_t).wait_recv()

    def each_block(k, body):
        if k == 0:
            body(z)
            return

        def one(d, carry):
            origin = z - (1 - 2 * d) * k

            @pl.when(exists(origin))
            def _():
                body(origin)

            return carry

        lax.fori_loop(0, 2, one, 0)

    def early(b):
        gate = jnp.dot(slots[1, b], w[0], preferred_element_type=f32)
        up = jnp.dot(slots[1, b], w[1], preferred_element_type=f32)
        hidden_grad = jnp.dot(slots[2, b], w[2], preferred_element_type=f32)
        hid[0, b], hid[1, b], hid[2, b] = early_parts(gate, up, hidden_grad)

    def early_level(k):
        if k:
            whole(EARLY, k)
            whole(COT, k)
        each_block(k, early)

    step = width // 4

    def trade(o, b):
        return remote(part.at[o, b, half(1 - t), :], peer.at[o, b], tds.at[0], tdr.at[o, b], to_t)

    def late(b):
        gate = jnp.dot(slots[0, b], w[0], preferred_element_type=f32)
        up = jnp.dot(slots[0, b], w[1], preferred_element_type=f32)
        hidden = (jax.nn.silu(gate) * up).astype(bf16)
        for c in range(4):
            lanes = slice(c * step, (c + 1) * step)
            part[0, b, :, lanes] = contract_last(hidden, w[2, lanes, :]).astype(bf16)
        trade(0, b).start()

    def late_level(k):
        if k:
            whole(LATE, k)
        each_block(k, late)

    def input_grad(b):
        for c in range(4):
            lanes = slice(c * step, (c + 1) * step)
            part[1, b, :, lanes] = (
                contract_last(hid[0, b], w[0, lanes, :]) + contract_last(hid[1, b], w[1, lanes, :])
            ).astype(bf16)
        trade(1, b).start()

    fine = 16

    def traded(o, b):
        remote(peer.at[o, b], peer.at[o, b], tds.at[0], tdr.at[o, b], to_t).wait_recv()

    def chunks(body):
        def one(i, carry):
            body(i * fine)
            return carry

        lax.fori_loop(0, q // fine, one, 0)

    def own(o, b, start):
        return (
            part[o, b, span(t * q + start, fine, fine), :].astype(f32)
            + peer[o, b, span(start, fine, fine), :].astype(f32)
        )

    def sum_copy(o, d, b, device):
        return remote(rout.at[o, b], rin.at[d, o, b], rss.at[0], rsr.at[d, o, b], device)

    def sum_step(o, far, h):
        @pl.when(jnp.logical_or(z == h, z == nz - 1 - h))
        def _():
            up = jnp.where(z == h, 1, 0)
            d = 1 - up
            b = up * far + d * (nz - 1 - far)
            copy = sum_copy(o, d, b, layer(z + 2 * up - 1))
            traded(o, b)
            if h:
                copy.wait_recv()

            def add(start):
                piece_rows = span(start, fine, fine)
                value = own(o, b, start)
                if h:
                    value = value + rin[d, o, b, piece_rows, :].astype(f32)
                rout[o, b, piece_rows, :] = value.astype(bf16)

            chunks(add)
            copy.start()

    def sum_end(o):
        traded(o, z)
        for d in range(2):
            @pl.when(exists(z - step_of(d)))
            def _():
                sum_copy(o, d, z, to_t).wait_recv()

        def add(start):
            piece_rows = span(start, fine, fine)
            value = own(o, z, start)
            for d in range(2):
                value = value + jnp.where(
                    exists(z - step_of(d)), rin[d, o, z, piece_rows, :].astype(f32), 0.0
                )
            outs[o][span(t * q + start, fine, fine), :] = value.astype(bf16)

        chunks(add)
        mine = outs[o].at[half(t), :]
        go(remote(mine, mine, os_.at[o], or_.at[o], to_t))

    def grad_block(side, height, i):
        lanes = span((height * 2 + side) * dl, dl, dl)
        source = slots[2 if i == 2 else 1, :, :, lanes].reshape(nz * m, dl)
        return contract_first(source, hid[i].reshape(nz * m, u))

    def grad_send(k, i):
        gyo[k, i] = grad_block(1 - y, flip(z, k, nz), i).astype(bf16)
        remote(gyo.at[k, i], gyi.at[k, i], gys.at[0], gyr.at[k, i], to_y).start()

    def grad_own(k, i):
        gown[k, i] = grad_block(y, flip(z, k, nz), i)

    mine_rows, their_rows = span(r * hr, hr, hr), span((1 - r) * hr, hr, hr)

    def grad_x(k, i):
        remote(gyi.at[k, i], gyi.at[k, i], gys.at[0], gyr.at[k, i], to_y).wait_recv()
        gxo[k, i] = (gown[k, i, their_rows, :] + gyi[k, i, their_rows, :].astype(f32)).astype(bf16)
        remote(gxo.at[k, i], gxi.at[k, i], gxs.at[0], gxr.at[k, i], to_x).start()

    def cross_x(i):
        return remote(gyo.at[0, i], gyi.at[0, i], gys.at[0], gyr.at[0, i], to_x)

    def cross_y(i):
        return remote(gxo.at[0, i], gxi.at[0, i], gxs.at[0], gxr.at[0, i], to_y)

    def cross_send(i):
        for s, side in enumerate((y, 1 - y)):
            gboth[s, i] = grad_block(side, z, i)
            gyo[0, i, s * hr:(s + 1) * hr, :] = gboth[s, i, their_rows, :].astype(bf16)
        cross_x(i).start()

    def cross_turn(i):
        cross_x(i).wait_recv()
        gxo[0, i] = (gboth[1, i, mine_rows, :] + gyi[0, i, hr:, :].astype(f32)).astype(bf16)
        cross_y(i).start()

    def cross_end(i):
        cross_y(i).wait_recv()
        g_out[i, mine_rows, units(z)] = (
            gboth[0, i, mine_rows, :] + gyi[0, i, :hr, :].astype(f32) + gxi[0, i].astype(f32)
        ).astype(bf16)
        grad_back(0, i)

    def g_block(i, height, h):
        return g_out.at[i, span(h * hr, hr, hr), units(height)]

    def grad_z(k, i):
        remote(gxi.at[k, i], gxi.at[k, i], gxs.at[0], gxr.at[k, i], to_x).wait_recv()
        total = (
            gown[k, i, mine_rows, :] + gyi[k, i, mine_rows, :].astype(f32) + gxi[k, i].astype(f32)
        ).astype(bf16)
        gzo[k, i] = total
        remote(gzo.at[k, i], g_block(i, z, r), gzs.at[0], gzr.at[k, i], layer(flip(z, k, nz))).start()

    def g_copy(k, i, h):
        block = g_block(i, flip(z, k, nz), h)
        return remote(block, block, gfs.at[0], gfr.at[k, i], to_x)

    def grad_back(k, i):
        if k:
            block = g_block(i, flip(z, k, nz), r)
            remote(block, block, gzs.at[0], gzr.at[k, i], to_x).wait_recv()
        g_copy(k, i, r).start()
        grad_add(k, i, r)

    def grad_add(k, i, h):
        place = (span(h * hr, hr, hr), units(flip(z, k, nz)))
        news[i][place] += g_out[(i,) + place].astype(f32)

    def grad_last(k, i):
        g_copy(k, i, 1 - r).wait_recv()
        grad_add(k, i, 1 - r)

    def run(name, task, *args):
        with jax.named_scope(name + "_".join(str(a) for a in args if isinstance(a, int))):
            task(*args)

    def send_first():
        for copy in local_weights:
            copy.wait()
        for k in range(1, nz):
            send_weights(flip(z, k, nz), wzs.at[0], wzr.at[k], layer(flip(z, k, nz)))
        send_weights(z, wys.at[0], wyr.at[0, 0], to_y)
        for copy in local_tokens:
            copy.wait()
        send_own(EARLY)
        send_own(COT)
        send_own(LATE, True)
        for copy in local_own:
            copy.wait()

    run("send_first", send_first)
    run("relay", relay, 0)
    for k in range(1, nz):
        run("spread", spread, k)
        if k > 1:
            run("relay", relay, k - 1)
    run("take_e", take_on, EARLY, 1)
    run("relay", relay, last)
    run("take_c", take_on, COT, 1)
    for k in range(last):
        run("gathered", gathered, k)
    if last > 1:
        run("take_e", take_on, EARLY, 2)
    run("gathered", gathered, last)
    run("early", early_level, 0)
    if last > 1:
        run("take_c", take_on, COT, 2)
    for k in range(3, last):
        run("take_e", take_on, EARLY, k)
        run("take_c", take_on, COT, k)
    run("send_l", send_own, LATE, False)
    run("early", early_level, 1)
    if last > 1:
        run("input_grad", each_block, 0, input_grad)
        run("input_grad", each_block, 1, input_grad)
    for k in range(2, last):
        run("early", early_level, k)
        run("sum_e", sum_step, 1, k - 1, 0)
        run("input_grad", each_block, k, input_grad)
    if last > 2:
        run("sum_e", sum_step, 1, last - 1, 0)
        run("take_e", take_on, EARLY, last)
        run("take_c", take_on, COT, last)
    if last > 1:
        run("early", early_level, last)
    order = [(k, i) for k in range(last, 0, -1) for i in range(3)]
    def send_next(count):
        for _ in range(count):
            if to_send:
                run("grad_send", grad_send, *to_send.pop(0))

    def own_next(count):
        for _ in range(count):
            if to_own:
                run("grad_own", grad_own, *to_own.pop(0))

    to_send, to_own = list(order), list(order)
    send_next(1)
    run("cross_send", cross_send, 0)
    send_next(1)
    run("cross_send", cross_send, 1)
    if last == 1:
        run("input_grad", each_block, 0, input_grad)
    run("input_grad", each_block, last, input_grad)
    send_next(1)
    run("cross_send", cross_send, 2)
    send_next(1)
    if last == 2:
        run("sum_e", sum_step, 1, 1, 0)
    run("sum_e", sum_step, 1, last, 0)
    run("take_l", take_on, LATE, 1)
    send_next(1)
    own_next(2)
    for copy in local_sums:
        copy.wait()
    run("late", late_level, 0)
    run("late", late_level, 1)

    between = {}

    def place(j, *task):
        between.setdefault(j, []).append(task)

    count, late_sums = len(order), []
    for i in range(3):
        place(i, "cross_turn", cross_turn, i)
        place(i + 6, "cross_end", cross_end, i)
    for far in range(2, nz):
        place(far - 2, "take_l", take_on, LATE, far)
        place(far - 1, "late", late_level, far)
        place(far, "sum_l", sum_step, 0, far, 0)
        for h in range(1, far):
            place(2 * (far - 2) - 1 + 5 * (h - 1), "sum_e", sum_step, 1, far, h)
            late_sums.append((far + 3 + (6 if h > 1 else 1) * (h - 1), far, h))
    place(0, "sum_l", sum_step, 0, 1, 0)
    place(2 * last + 2, "sum_end_e", sum_end, 1)
    for j, (k, i) in enumerate(order):
        place(j + (5 if k == last else 6 if k > 1 else 4), "grad_back", grad_back, k, i)
    for j, far, h in late_sums:
        place(j, "sum_l", sum_step, 0, far, h)
    place(count + 3, "sum_end_l", sum_end, 0)
    for j in range(min(min(between), -1), max(max(between), count) + 1):
        if 0 <= j < count:
            own_next(1)
            run("grad_x", grad_x, *order[j])
            send_next(1)
        if 1 <= j <= count:
            run("grad_z", grad_z, *order[j - 1])
        for name, task, *args in between.get(j, ()):
            run(name, task, *args)
    for k, i in [(0, 0), (0, 1), (0, 2)] + order:
        run("grad_last", grad_last, k, i)
    def finish():
        for o in range(2):
            other = outs[o].at[half(1 - t), :]
            remote(other, other, os_.at[o], or_.at[o], to_t).wait_recv()

    def drain():
        def sent(block, sem):
            remote(block, block, sem.at[0], sem.at[0], to_t).wait_send()

        sent(w.at[:, pl.ds(0, last * hr), :], wzs)
        sent(w.at[:, pl.ds(0, (last + nz // 2) * hr), :], wxs)
        sent(w.at[:, pl.ds(0, (nz + nz // 2) * hr), :], wys)
        sent(slots.at[:, pl.ds(0, last), pl.ds(0, q), :], cs)
        sent(peer, tds)
        sent(rout.at[:, pl.ds(0, last)], rss)
        sent(gyo, gys)
        sent(gxo, gxs)
        sent(gzo.at[pl.ds(1, last)], gzs)
        sent(gxo, gfs)
        for condition, copy in pending:
            if condition is None:
                copy.wait_send()
            else:
                @pl.when(condition)
                def _():
                    copy.wait_send()

    run("finish", finish)
    run("drain", drain)


def close_kernel(*refs):
    sems = refs[-1]
    count = (len(refs) - 1) // 2
    copies = [pltpu.make_async_copy(refs[i], refs[count + i], sems.at[i]) for i in range(count)]
    for copy in copies:
        copy.start()
    for copy in copies:
        copy.wait()


def close(*arrays):
    return pl.pallas_call(
        close_kernel,
        out_shape=tuple(jax.ShapeDtypeStruct(a.shape, a.dtype) for a in arrays),
        in_specs=[VMEM] * len(arrays),
        out_specs=(HBM,) * len(arrays),
        scratch_shapes=[dma(len(arrays))],
        compiler_params=pltpu.CompilerParams(vmem_limit_bytes=8 * 2**20),
        name="close",
    )(*arrays)


VMEM = pl.BlockSpec(memory_space=pltpu.VMEM)
HBM = pl.BlockSpec(memory_space=pltpu.HBM)


def dma(*shape):
    return pltpu.SemaphoreType.DMA(shape)


def split_hidden(
    n,
    later_input,
    earlier_input,
    cotangent,
    gate_weight,
    up_weight,
    down_weight,
    gate_sum,
    up_sum,
    down_sum,
):
    bf16, f32 = jnp.bfloat16, jnp.float32
    m, width = later_input.shape
    dl, ff = gate_weight.shape
    nz = n // 2
    u, q, hr = ff // nz, m // 2, dl // 2
    results = pl.pallas_call(
        functools.partial(fused_kernel, nz),
        out_shape=(
            jax.ShapeDtypeStruct((m, width), bf16),
            jax.ShapeDtypeStruct((m, width), bf16),
            jax.ShapeDtypeStruct((dl, ff), f32),
            jax.ShapeDtypeStruct((dl, ff), f32),
            jax.ShapeDtypeStruct((dl, ff), f32),
        ),
        in_specs=[HBM] * 9,
        out_specs=(VMEM,) * 5,
        scratch_shapes=[
            pltpu.VMEM((3, nz, m, width), bf16),
            pltpu.VMEM((3, dl, ff), bf16),
            pltpu.VMEM((3, width, u), bf16),
            pltpu.VMEM((3, dl, ff), bf16),
            pltpu.VMEM((3, nz, m, u), bf16),
            pltpu.VMEM((2, nz, m, width), bf16),
            pltpu.VMEM((2, nz, q, width), bf16),
            pltpu.VMEM((2, 2, nz, q, width), bf16),
            pltpu.VMEM((2, nz, q, width), bf16),
            pltpu.VMEM((nz, 3, dl, u), f32),
            pltpu.VMEM((2, 3, dl, u), f32),
            pltpu.VMEM((nz, 3, dl, u), bf16),
            pltpu.VMEM((nz, 3, dl, u), bf16),
            pltpu.VMEM((nz, 3, hr, u), bf16),
            pltpu.VMEM((nz, 3, hr, u), bf16),
            pltpu.VMEM((nz, 3, hr, u), bf16),
        ]
        + [dma(3)] * 4
        + [dma(1), dma(nz), dma(1), dma(nz, 2), dma(1), dma(nz, 2)]
        + [dma(3, 2), dma(3, max(nz - 1, 1), 2), dma(3, nz), dma(1), dma(3, nz)]
        + [dma(1), dma(2, nz), dma(1), dma(2, 2, nz), dma(2), dma(2)]
        + [dma(1), dma(nz, 3)] * 4,
        compiler_params=pltpu.CompilerParams(
            collective_id=0, has_side_effects=True, vmem_limit_bytes=46 * 2**20
        ),
        name="fused",
    )(
        *(
            pltpu.with_memory_space_constraint(a, pltpu.HBM)
            for a in (later_input, earlier_input, cotangent, gate_weight, up_weight, down_weight, gate_sum, up_sum, down_sum)
        )
    )
    return close(*results)


def early_parts(gate_early, up_early, hidden_grad):
    sigmoid_gate = jax.nn.sigmoid(gate_early)
    silu_early = gate_early * sigmoid_gate
    gate_grad = (
        hidden_grad * up_early * sigmoid_gate * (1.0 + gate_early * (1.0 - sigmoid_gate))
    ).astype(jnp.bfloat16)
    up_grad = (hidden_grad * silu_early).astype(jnp.bfloat16)
    hidden_early = (silu_early * up_early).astype(jnp.bfloat16)
    return gate_grad, up_grad, hidden_early


def contract_last(first, second):
    return lax.dot_general(
        first, second, (((1,), (1,)), ((), ())), preferred_element_type=jnp.float32
    )


def contract_first(first, second):
    return lax.dot_general(
        first, second, (((0,), (0,)), ((), ())), preferred_element_type=jnp.float32
    )


def per_device(
    later_input,
    earlier_input,
    cotangent,
    gate_weight,
    up_weight,
    down_weight,
    gate_sum,
    up_sum,
    down_sum,
):
    gate_full, up_full, down_full = (
        lax.all_gather(gate_weight, "fs", axis=0, tiled=True),
        lax.all_gather(up_weight, "fs", axis=0, tiled=True),
        lax.all_gather(down_weight, "fs", axis=0, tiled=True),
    )
    gate_late = jnp.dot(later_input, gate_full, preferred_element_type=jnp.float32)
    up_late = jnp.dot(later_input, up_full, preferred_element_type=jnp.float32)
    hidden_late = (jax.nn.silu(gate_late) * up_late).astype(jnp.bfloat16)
    partial_late = contract_last(hidden_late, down_full)
    later_output = lax.psum(partial_late.astype(jnp.bfloat16), "tp")
    gate_early = jnp.dot(earlier_input, gate_full, preferred_element_type=jnp.float32)
    up_early = jnp.dot(earlier_input, up_full, preferred_element_type=jnp.float32)
    hidden_grad = jnp.dot(cotangent, down_full, preferred_element_type=jnp.float32)
    sigmoid_gate = jax.nn.sigmoid(gate_early)
    silu_early = gate_early * sigmoid_gate
    gate_grad = (
        hidden_grad * up_early * sigmoid_gate * (1.0 + gate_early * (1.0 - sigmoid_gate))
    ).astype(jnp.bfloat16)
    up_grad = (hidden_grad * silu_early).astype(jnp.bfloat16)
    hidden_early = (silu_early * up_early).astype(jnp.bfloat16)
    partial_early = contract_last(gate_grad, gate_full) + contract_last(up_grad, up_full)
    earlier_input_grad = lax.psum(partial_early.astype(jnp.bfloat16), "tp")
    columns, cot_columns = (
        lax.all_to_all(earlier_input, "fs", split_axis=1, concat_axis=0, tiled=True),
        lax.all_to_all(cotangent, "fs", split_axis=1, concat_axis=0, tiled=True),
    )
    gate_local = contract_first(columns, lax.all_gather(gate_grad, "fs", axis=0, tiled=True))
    up_local = contract_first(columns, lax.all_gather(up_grad, "fs", axis=0, tiled=True))
    down_local = contract_first(cot_columns, lax.all_gather(hidden_early, "fs", axis=0, tiled=True))
    gate_total, up_total, down_total = (
        lax.psum(gate_local.astype(jnp.bfloat16), "rep").astype(jnp.float32),
        lax.psum(up_local.astype(jnp.bfloat16), "rep").astype(jnp.float32),
        lax.psum(down_local.astype(jnp.bfloat16), "rep").astype(jnp.float32),
    )
    return (
        later_output,
        earlier_input_grad,
        gate_sum + gate_total,
        up_sum + up_total,
        down_sum + down_total,
    )


def solution(mesh):
    placed = (
        P(("rep", "fs"), None),
        P(("rep", "fs"), None),
        P(("rep", "fs"), None),
        P("fs", "tp"),
        P("fs", "tp"),
        P("fs", "tp"),
        P("fs", "tp"),
        P("fs", "tp"),
        P("fs", "tp"),
    )
    reps, shards, blocks = (mesh.shape[axis] for axis in ("rep", "fs", "tp"))

    def chosen(*arrays):
        rows = arrays[0].shape[0]
        depth, units = arrays[3].shape
        layers = shards // 2
        fits = (
            reps == 2
            and blocks == 2
            and layers >= 2
            and shards == 2 * layers
            and layers & (layers - 1) == 0
            and units % (layers * 128) == 0
            and depth % 128 == 0
            and rows % 64 == 0
            and arrays[0].shape[1] % 512 == 0
            and arrays[0].shape[1] == depth * shards
        )
        return split_hidden(shards, *arrays) if fits else per_device(*arrays)

    return jax.shard_map(
        chosen,
        mesh=mesh,
        in_specs=placed,
        out_specs=(
            P(("rep", "fs"), None),
            P(("rep", "fs"), None),
            P("fs", "tp"),
            P("fs", "tp"),
            P("fs", "tp"),
        ),
        check_vma=False,
    )
```

```python
import functools

import jax
import jax.numpy as jnp
from jax import lax
from jax.experimental import pallas as pl
from jax.experimental.pallas import tpu as pltpu
from jax.sharding import PartitionSpec as P

MESH = pl.DeviceIdType.MESH


def flip(index, k, n):
    out, bit = 0, 1
    while bit < n:
        digit = lax.rem(index // bit, 2)
        out = out + bit * ((1 - digit) if k & bit else digit)
        bit *= 2
    return out


def span(start, size, step):
    return pl.ds(pl.multiple_of(start, step), size)


def remote(source, target, send, recv, device):
    return pltpu.make_async_remote_copy(
        src_ref=source,
        dst_ref=target,
        send_sem=send,
        recv_sem=recv,
        device_id=device,
        device_id_type=MESH,
    )


EARLY, COT, LATE = 0, 1, 2


def fused_kernel(
    nz, later, earlier, cot, gw, uw, dw, gsum, usum, dsum, late_out, early_out, gnew, unew, dnew,
    slots, wt, w, g_out, hid, part, peer, rin, rout, gown, gside, gother, gyo, gyi, gxo, gxi, gzo,
    lts, lws, los, lns, wzs, wzr, wxs, wxr, wys, wyr, aos, ags, agr, cs, cr,
    tds, tdr, rss, rsr, os_, or_, gys, gyr, gxs, gxr, gzs, gzr, gfs, gfr,
):
    r, f, t = lax.axis_index("rep"), lax.axis_index("fs"), lax.axis_index("tp")
    y, z = lax.rem(f, 2), f // 2
    m, width = later.shape
    q = m // 2
    dl, u = gw.shape[0], w.shape[2]
    hr, last = dl // 2, nz - 1
    f32, bf16 = jnp.float32, jnp.bfloat16
    outs = (late_out, early_out)
    to_x, to_y, to_t = {"rep": 1 - r}, {"fs": z * 2 + 1 - y}, {"tp": 1 - t}

    def layer(height):
        return {"fs": height * 2 + y}

    def units(height):
        return span(height * u, u, u)

    slot_of = (1, 2, 0)
    local_tokens = [
        pltpu.make_async_copy(source, slots.at[slot_of[g], z], lts.at[g])
        for g, source in enumerate((earlier, cot, later))
    ]
    local_weights = [pltpu.make_async_copy(source, wt.at[i], lws.at[i]) for i, source in enumerate((gw, uw, dw))]
    local_own = [
        pltpu.make_async_copy(source.at[:, units(z)], w.at[i, span((z * 2 + y) * dl, dl, dl), :], los.at[i])
        for i, source in enumerate((gw, uw, dw))
    ]
    news = (gnew, unew, dnew)
    local_sums = [pltpu.make_async_copy(source, news[i], lns.at[i]) for i, source in enumerate((gsum, usum, dsum))]
    for copy in local_weights + local_tokens + local_own + local_sums:
        copy.start()

    barrier = pltpu.get_barrier_semaphore()
    for device in [layer(flip(z, k, nz)) for k in range(1, nz)] + [to_x, to_y, to_t]:
        pl.semaphore_signal(barrier, inc=1, device_id=device, device_id_type=MESH)
    pl.semaphore_wait(barrier, nz + 2)

    pending = []

    def go(copy):
        copy.start()
        pending.append((None, copy))

    def when_go(condition, copy):
        @pl.when(condition)
        def _():
            copy.start()

        pending.append((condition, copy))

    def rows(side, height, h):
        return span((height * 2 + side) * dl + h * hr, hr, hr)

    def piece(side, height, h):
        return w.at[:, rows(side, height, h), :]

    def send_weights(height, send, recv, device):
        remote(wt.at[:, span(r * hr, hr, hr), units(height)], piece(y, z, r), send, recv, device).start()

    def wx(k, a, block):
        return remote(block, block, wxs.at[0], wxr.at[k, a], to_x)

    def wy(k, a, block):
        return remote(block, block, wys.at[0], wyr.at[k, a], to_y)

    def spread(k):
        block = piece(y, flip(z, k, nz), r)
        remote(block, block, wzs.at[0], wzr.at[k], to_x).wait_recv()
        wx(k, 0, block).start()
        wy(k, 0, block).start()

    def relay(k):
        height = flip(z, k, nz)
        if k % 2:
            block = piece(y, height, 1 - r)
            wx(k, 0, block).wait_recv()
            wy(k, 1, block).start()
        else:
            block = piece(1 - y, height, r)
            wy(k, 0, block).wait_recv()
            wx(k, 1, block).start()

    def gathered(k):
        height = flip(z, k, nz)
        if k % 2:
            wy(k, 0, piece(1 - y, height, r)).wait_recv()
            wy(k, 1, piece(1 - y, height, 1 - r)).wait_recv()
        else:
            if k:
                wx(k, 0, piece(y, height, 1 - r)).wait_recv()
            wx(k, 1, piece(1 - y, height, 1 - r)).wait_recv()

    def half(core):
        return span(core * q, q, q)

    def block_of(g, origin, core):
        return slots.at[slot_of[g], origin, half(core), :]

    def step_of(d):
        return 1 - 2 * d

    def exists(height):
        return jnp.logical_and(height >= 0, height < nz)

    def send_own(g, ends=None):
        for d in range(2):
            target = z + step_of(d)
            block = block_of(g, z, t)
            at_end = z == (last if d else 0)
            chosen = exists(target)
            if ends is not None:
                chosen = jnp.logical_and(chosen, at_end if ends else jnp.logical_not(at_end))
            when_go(chosen, remote(block, block, aos.at[g, d], agr.at[g, z], layer(target)))

    def take_on(g, k, ends=None):
        for d in range(2):
            origin, target = z - step_of(d) * k, z + step_of(d)
            block = block_of(g, origin, t)
            ahead = remote(block, block, ags.at[g, min(k, last - 1), d], agr.at[g, origin], layer(target))
            chosen = exists(origin)
            if ends is not None:
                at_end = origin == (last if d else 0)
                chosen = jnp.logical_and(chosen, at_end if ends else jnp.logical_not(at_end))

            @pl.when(chosen)
            def _():
                ahead.wait_recv()

            if k < last:
                when_go(jnp.logical_and(chosen, exists(target)), ahead)

            @pl.when(chosen)
            def _():
                remote(block, block, cs.at[0], cr.at[g, origin], to_t).start()

    def whole(g, k):
        for d in range(2):
            origin = z - step_of(d) * k
            block = block_of(g, origin, 1 - t)

            @pl.when(exists(origin))
            def _():
                remote(block, block, cs.at[0], cr.at[g, origin], to_t).wait_recv()

    def each_block(k, body):
        if k == 0:
            body(z)
            return

        def one(d, carry):
            origin = z - (1 - 2 * d) * k

            @pl.when(exists(origin))
            def _():
                body(origin)

            return carry

        lax.fori_loop(0, 2, one, 0)

    def early(b):
        gate = jnp.dot(slots[1, b], w[0], preferred_element_type=f32)
        up = jnp.dot(slots[1, b], w[1], preferred_element_type=f32)
        hidden_grad = jnp.dot(slots[2, b], w[2], preferred_element_type=f32)
        hid[0, b], hid[1, b], hid[2, b] = early_parts(gate, up, hidden_grad)

    def early_level(k):
        if k:
            whole(EARLY, k)
            whole(COT, k)
        each_block(k, early)

    step = width // 4

    def trade(o, b):
        return remote(part.at[o, b, half(1 - t), :], peer.at[o, b], tds.at[0], tdr.at[o, b], to_t)

    def late(b):
        gate = jnp.dot(slots[0, b], w[0], preferred_element_type=f32)
        up = jnp.dot(slots[0, b], w[1], preferred_element_type=f32)
        hidden = (jax.nn.silu(gate) * up).astype(bf16)
        for c in range(4):
            lanes = slice(c * step, (c + 1) * step)
            part[0, b, :, lanes] = contract_last(hidden, w[2, lanes, :]).astype(bf16)
        trade(0, b).start()

    def late_level(k):
        if k:
            whole(LATE, k)
        each_block(k, late)

    def input_grad(b):
        for c in range(4):
            lanes = slice(c * step, (c + 1) * step)
            part[1, b, :, lanes] = (
                contract_last(hid[0, b], w[0, lanes, :]) + contract_last(hid[1, b], w[1, lanes, :])
            ).astype(bf16)
        trade(1, b).start()

    fine = 16

    def traded(o, b):
        remote(peer.at[o, b], peer.at[o, b], tds.at[0], tdr.at[o, b], to_t).wait_recv()

    def chunks(body):
        def one(i, carry):
            body(i * fine)
            return carry

        lax.fori_loop(0, q // fine, one, 0)

    def own(o, b, start):
        return (
            part[o, b, span(t * q + start, fine, fine), :].astype(f32)
            + peer[o, b, span(start, fine, fine), :].astype(f32)
        )

    def sum_copy(o, d, b, device):
        return remote(rout.at[o, b], rin.at[d, o, b], rss.at[0], rsr.at[d, o, b], device)

    def sum_step(o, far, h):
        @pl.when(jnp.logical_or(z == h, z == nz - 1 - h))
        def _():
            up = jnp.where(z == h, 1, 0)
            d = 1 - up
            b = up * far + d * (nz - 1 - far)
            copy = sum_copy(o, d, b, layer(z + 2 * up - 1))
            traded(o, b)
            if h:
                copy.wait_recv()

            def add(start):
                piece_rows = span(start, fine, fine)
                value = own(o, b, start)
                if h:
                    value = value + rin[d, o, b, piece_rows, :].astype(f32)
                rout[o, b, piece_rows, :] = value.astype(bf16)

            chunks(add)
            copy.start()

    def sum_end(o):
        traded(o, z)
        for d in range(2):
            @pl.when(exists(z - step_of(d)))
            def _():
                sum_copy(o, d, z, to_t).wait_recv()

        def add(start):
            piece_rows = span(start, fine, fine)
            value = own(o, z, start)
            for d in range(2):
                value = value + jnp.where(
                    exists(z - step_of(d)), rin[d, o, z, piece_rows, :].astype(f32), 0.0
                )
            outs[o][span(t * q + start, fine, fine), :] = value.astype(bf16)

        chunks(add)
        mine = outs[o].at[half(t), :]
        go(remote(mine, mine, os_.at[o], or_.at[o], to_t))

    def grad_block(side, height, i):
        lanes = span((height * 2 + side) * dl, dl, dl)
        source = slots[2 if i == 2 else 1, :, :, lanes].reshape(nz * m, dl)
        return contract_first(source, hid[i].reshape(nz * m, u))

    def grad_send(k, i):
        gyo[k, i] = grad_block(1 - y, flip(z, k, nz), i).astype(bf16)
        remote(gyo.at[k, i], gyi.at[k, i], gys.at[0], gyr.at[k, i], to_y).start()

    def grad_own(k, i):
        gown[k, i] = grad_block(y, flip(z, k, nz), i)

    mine_rows, their_rows = span(r * hr, hr, hr), span((1 - r) * hr, hr, hr)

    def grad_x(k, i):
        remote(gyi.at[k, i], gyi.at[k, i], gys.at[0], gyr.at[k, i], to_y).wait_recv()
        gxo[k, i] = (gown[k, i, their_rows, :] + gyi[k, i, their_rows, :].astype(f32)).astype(bf16)
        remote(gxo.at[k, i], gxi.at[k, i], gxs.at[0], gxr.at[k, i], to_x).start()

    def cross_x(k, i):
        return remote(gyo.at[k, i], gyi.at[k, i], gys.at[0], gyr.at[k, i], to_x)

    def cross_y(k, i):
        return remote(gxo.at[k, i], gxi.at[k, i], gxs.at[0], gxr.at[k, i], to_y)

    def cross_send(k, i, c):
        gown[k, i] = grad_block(y, flip(z, k, nz), i)
        gyo[k, i, :hr, :] = gown[k, i, their_rows, :].astype(bf16)
        gside[...] = grad_block(1 - y, flip(z, k, nz), i)
        gyo[k, i, hr:, :] = gside[their_rows, :].astype(bf16)
        gother[c] = gside[mine_rows, :]
        cross_x(k, i).start()

    def cross_turn(k, i, c):
        cross_x(k, i).wait_recv()
        gxo[k, i] = (gother[c] + gyi[k, i, hr:, :].astype(f32)).astype(bf16)
        cross_y(k, i).start()

    def cross_end(k, i, c):
        cross_y(k, i).wait_recv()
        total = (gown[k, i, mine_rows, :] + gyi[k, i, :hr, :].astype(f32) + gxi[k, i].astype(f32)).astype(bf16)
        if k:
            gzo[k, i] = total
            grad_onward(k, i)
        else:
            g_out[i, mine_rows, units(z)] = total
            grad_back(k, i)

    def grad_onward(k, i):
        remote(gzo.at[k, i], g_block(i, z, r), gzs.at[0], gzr.at[k, i], layer(flip(z, k, nz))).start()

    def g_block(i, height, h):
        return g_out.at[i, span(h * hr, hr, hr), units(height)]

    def grad_z(k, i):
        remote(gxi.at[k, i], gxi.at[k, i], gxs.at[0], gxr.at[k, i], to_x).wait_recv()
        total = (
            gown[k, i, mine_rows, :] + gyi[k, i, mine_rows, :].astype(f32) + gxi[k, i].astype(f32)
        ).astype(bf16)
        gzo[k, i] = total
        grad_onward(k, i)

    def g_copy(k, i, h):
        block = g_block(i, flip(z, k, nz), h)
        return remote(block, block, gfs.at[0], gfr.at[k, i], to_x)

    def grad_back(k, i):
        if k:
            block = g_block(i, flip(z, k, nz), r)
            remote(block, block, gzs.at[0], gzr.at[k, i], to_x).wait_recv()
        g_copy(k, i, r).start()
        grad_add(k, i, r)

    def grad_add(k, i, h):
        place = (span(h * hr, hr, hr), units(flip(z, k, nz)))
        news[i][place] += g_out[(i,) + place].astype(f32)

    def grad_last(k, i):
        g_copy(k, i, 1 - r).wait_recv()
        grad_add(k, i, 1 - r)

    def run(name, task, *args):
        with jax.named_scope(name + "_".join(str(a) for a in args if isinstance(a, int))):
            task(*args)

    def send_first():
        for copy in local_weights:
            copy.wait()
        for k in range(1, nz):
            send_weights(flip(z, k, nz), wzs.at[0], wzr.at[k], layer(flip(z, k, nz)))
        send_weights(z, wys.at[0], wyr.at[0, 0], to_y)
        for copy in local_tokens:
            copy.wait()
        send_own(EARLY)
        send_own(COT)
        send_own(LATE, True)
        for copy in local_own:
            copy.wait()

    run("send_first", send_first)
    run("relay", relay, 0)
    for k in range(1, nz):
        run("spread", spread, k)
        if k > 1:
            run("relay", relay, k - 1)
    run("take_e", take_on, EARLY, 1)
    run("relay", relay, last)
    run("take_c", take_on, COT, 1)
    for k in range(last):
        run("gathered", gathered, k)
    if last > 1:
        run("take_e", take_on, EARLY, 2)
    run("gathered", gathered, last)
    run("early", early_level, 0)
    if last > 1:
        run("take_c", take_on, COT, 2)
    for k in range(3, last):
        run("take_e", take_on, EARLY, k)
        run("take_c", take_on, COT, k)
    run("send_l", send_own, LATE, False)
    run("take_l_end", take_on, LATE, 1, True)
    for k in range(last - 1, 0, -1):
        run("early", early_level, k)
        if 1 < k + 1 < last:
            run("sum_e", sum_step, 1, k + 1, 0)
        run("input_grad", each_block, k, input_grad)
    if last > 2:
        run("take_e", take_on, EARLY, last)
        run("take_c", take_on, COT, last)
    if last == 1:
        run("early", early_level, 1)
    if last > 1:
        run("early", early_level, last)
    crossing = [(0, 0), (0, 1), (0, 2)] + [(1, i) for i in range(1)]
    order = [(k, i) for k in range(last, 0, -1) for i in range(3) if (k, i) not in crossing]
    def send_next(count):
        for _ in range(count):
            if to_send:
                run("grad_send", grad_send, *to_send.pop(0))

    def wait_sums():
        for copy in local_sums:
            copy.wait()

    def own_next(count):
        for _ in range(count):
            if to_own:
                run("grad_own", grad_own, *to_own.pop(0))

    to_send, to_own = list(order), list(order)
    send_next(1)
    run("cross_send", cross_send, *crossing[0], 0)
    send_next(1)
    run("cross_send", cross_send, *crossing[1], 1)
    run("input_grad", each_block, last, input_grad)
    send_next(2)
    run("take_l", take_on, LATE, 1, False)
    run("sum_e", sum_step, 1, last, 0)
    if last > 1:
        run("sum_e", sum_step, 1, 1, 0)
    run("input_grad", each_block, 0, input_grad)
    send_next(1)
    own_next(2)

    between = {}

    def place(j, *task):
        between.setdefault(j, []).append(task)

    count = len(order)
    for far in range(2, nz):
        for h in range(1, far):
            place(2 * far - 5 + 5 * (h - 1), "sum_e", sum_step, 1, far, h)
    place(-1, "late", late_level, 1)
    if last > 1:
        place(-1, "take_l", take_on, LATE, 2)
    place(-1, "late", late_level, 0)
    for far in range(3, nz):
        place(far - 2, "take_l", take_on, LATE, far)
    for far in range(last, 0, -1):
        if far > 1:
            place(2 * (last - far) + 1, "late", late_level, far)
        place(last - far + 2, "sum_l", sum_step, 0, far, 0)
        for h in range(1, far):
            place(5 + 2 * (last - far) + 5 * (h - 1), "sum_l", sum_step, 0, far, h)
    for c, (k, i) in enumerate(crossing):
        if c > 1:
            place(c, "cross_send", cross_send, k, i, c)
        place((0, 2, 5, 6, 7, 8)[c], "cross_turn", cross_turn, k, i, c)
        place((6, 7, 8, 8, 9, 9)[c], "cross_end", cross_end, k, i, c)
        if k:
            place((6, 7, 8, 8, 9, 9)[c] + 3, "grad_back", grad_back, k, i)
    place(2 * last + 2, "sum_end_e", sum_end, 1)
    for j, (k, i) in enumerate(order):
        place(j + (5 if k > 1 else 4), "grad_back", grad_back, k, i)
    place(12, "sum_end_l", sum_end, 0)
    place(-1, "sums", wait_sums)
    for j in range(min(min(between), -1), max(max(between), count) + 1):
        if 0 <= j < count:
            own_next(1)
            run("grad_x", grad_x, *order[j])
            send_next(1)
        if 1 <= j <= count:
            run("grad_z", grad_z, *order[j - 1])
        for name, task, *args in between.get(j, ()):
            run(name, task, *args)
    for k, i in crossing[:3] + order + crossing[3:]:
        run("grad_last", grad_last, k, i)
    def finish():
        for o in range(2):
            other = outs[o].at[half(1 - t), :]
            remote(other, other, os_.at[o], or_.at[o], to_t).wait_recv()

    def drain():
        def sent(block, sem):
            remote(block, block, sem.at[0], sem.at[0], to_t).wait_send()

        sent(w.at[:, pl.ds(0, last * hr), :], wzs)
        sent(w.at[:, pl.ds(0, (last + nz // 2) * hr), :], wxs)
        sent(w.at[:, pl.ds(0, (nz + nz // 2) * hr), :], wys)
        sent(slots.at[:, pl.ds(0, last), pl.ds(0, q), :], cs)
        sent(peer, tds)
        sent(rout.at[:, pl.ds(0, last)], rss)
        sent(gyo, gys)
        sent(gxo, gxs)
        sent(gzo.at[pl.ds(1, last)], gzs)
        sent(gxo, gfs)
        for condition, copy in pending:
            if condition is None:
                copy.wait_send()
            else:
                @pl.when(condition)
                def _():
                    copy.wait_send()

    run("finish", finish)
    run("drain", drain)


def close_kernel(*refs):
    sems = refs[-1]
    count = (len(refs) - 1) // 2
    copies = [pltpu.make_async_copy(refs[i], refs[count + i], sems.at[i]) for i in range(count)]
    for copy in copies:
        copy.start()
    for copy in copies:
        copy.wait()


def close(*arrays):
    return pl.pallas_call(
        close_kernel,
        out_shape=tuple(jax.ShapeDtypeStruct(a.shape, a.dtype) for a in arrays),
        in_specs=[VMEM] * len(arrays),
        out_specs=(HBM,) * len(arrays),
        scratch_shapes=[dma(len(arrays))],
        compiler_params=pltpu.CompilerParams(vmem_limit_bytes=8 * 2**20),
        name="close",
    )(*arrays)


VMEM = pl.BlockSpec(memory_space=pltpu.VMEM)
HBM = pl.BlockSpec(memory_space=pltpu.HBM)


def dma(*shape):
    return pltpu.SemaphoreType.DMA(shape)


def split_hidden(
    n,
    later_input,
    earlier_input,
    cotangent,
    gate_weight,
    up_weight,
    down_weight,
    gate_sum,
    up_sum,
    down_sum,
):
    bf16, f32 = jnp.bfloat16, jnp.float32
    m, width = later_input.shape
    dl, ff = gate_weight.shape
    nz = n // 2
    u, q, hr = ff // nz, m // 2, dl // 2
    results = pl.pallas_call(
        functools.partial(fused_kernel, nz),
        out_shape=(
            jax.ShapeDtypeStruct((m, width), bf16),
            jax.ShapeDtypeStruct((m, width), bf16),
            jax.ShapeDtypeStruct((dl, ff), f32),
            jax.ShapeDtypeStruct((dl, ff), f32),
            jax.ShapeDtypeStruct((dl, ff), f32),
        ),
        in_specs=[HBM] * 9,
        out_specs=(VMEM,) * 5,
        scratch_shapes=[
            pltpu.VMEM((3, nz, m, width), bf16),
            pltpu.VMEM((3, dl, ff), bf16),
            pltpu.VMEM((3, width, u), bf16),
            pltpu.VMEM((3, dl, ff), bf16),
            pltpu.VMEM((3, nz, m, u), bf16),
            pltpu.VMEM((2, nz, m, width), bf16),
            pltpu.VMEM((2, nz, q, width), bf16),
            pltpu.VMEM((2, 2, nz, q, width), bf16),
            pltpu.VMEM((2, nz, q, width), bf16),
            pltpu.VMEM((nz, 3, dl, u), f32),
            pltpu.VMEM((dl, u), f32),
            pltpu.VMEM((6, hr, u), f32),
            pltpu.VMEM((nz, 3, dl, u), bf16),
            pltpu.VMEM((nz, 3, dl, u), bf16),
            pltpu.VMEM((nz, 3, hr, u), bf16),
            pltpu.VMEM((nz, 3, hr, u), bf16),
            pltpu.VMEM((nz, 3, hr, u), bf16),
        ]
        + [dma(3)] * 4
        + [dma(1), dma(nz), dma(1), dma(nz, 2), dma(1), dma(nz, 2)]
        + [dma(3, 2), dma(3, max(nz - 1, 1), 2), dma(3, nz), dma(1), dma(3, nz)]
        + [dma(1), dma(2, nz), dma(1), dma(2, 2, nz), dma(2), dma(2)]
        + [dma(1), dma(nz, 3)] * 4,
        compiler_params=pltpu.CompilerParams(
            collective_id=0, has_side_effects=True, vmem_limit_bytes=46 * 2**20
        ),
        name="fused",
    )(
        *(
            pltpu.with_memory_space_constraint(a, pltpu.HBM)
            for a in (later_input, earlier_input, cotangent, gate_weight, up_weight, down_weight, gate_sum, up_sum, down_sum)
        )
    )
    return close(*results)


def early_parts(gate_early, up_early, hidden_grad):
    sigmoid_gate = jax.nn.sigmoid(gate_early)
    silu_early = gate_early * sigmoid_gate
    gate_grad = (
        hidden_grad * up_early * sigmoid_gate * (1.0 + gate_early * (1.0 - sigmoid_gate))
    ).astype(jnp.bfloat16)
    up_grad = (hidden_grad * silu_early).astype(jnp.bfloat16)
    hidden_early = (silu_early * up_early).astype(jnp.bfloat16)
    return gate_grad, up_grad, hidden_early


def contract_last(first, second):
    return lax.dot_general(
        first, second, (((1,), (1,)), ((), ())), preferred_element_type=jnp.float32
    )


def contract_first(first, second):
    return lax.dot_general(
        first, second, (((0,), (0,)), ((), ())), preferred_element_type=jnp.float32
    )


def per_device(
    later_input,
    earlier_input,
    cotangent,
    gate_weight,
    up_weight,
    down_weight,
    gate_sum,
    up_sum,
    down_sum,
):
    gate_full, up_full, down_full = (
        lax.all_gather(gate_weight, "fs", axis=0, tiled=True),
        lax.all_gather(up_weight, "fs", axis=0, tiled=True),
        lax.all_gather(down_weight, "fs", axis=0, tiled=True),
    )
    gate_late = jnp.dot(later_input, gate_full, preferred_element_type=jnp.float32)
    up_late = jnp.dot(later_input, up_full, preferred_element_type=jnp.float32)
    hidden_late = (jax.nn.silu(gate_late) * up_late).astype(jnp.bfloat16)
    partial_late = contract_last(hidden_late, down_full)
    later_output = lax.psum(partial_late.astype(jnp.bfloat16), "tp")
    gate_early = jnp.dot(earlier_input, gate_full, preferred_element_type=jnp.float32)
    up_early = jnp.dot(earlier_input, up_full, preferred_element_type=jnp.float32)
    hidden_grad = jnp.dot(cotangent, down_full, preferred_element_type=jnp.float32)
    sigmoid_gate = jax.nn.sigmoid(gate_early)
    silu_early = gate_early * sigmoid_gate
    gate_grad = (
        hidden_grad * up_early * sigmoid_gate * (1.0 + gate_early * (1.0 - sigmoid_gate))
    ).astype(jnp.bfloat16)
    up_grad = (hidden_grad * silu_early).astype(jnp.bfloat16)
    hidden_early = (silu_early * up_early).astype(jnp.bfloat16)
    partial_early = contract_last(gate_grad, gate_full) + contract_last(up_grad, up_full)
    earlier_input_grad = lax.psum(partial_early.astype(jnp.bfloat16), "tp")
    columns, cot_columns = (
        lax.all_to_all(earlier_input, "fs", split_axis=1, concat_axis=0, tiled=True),
        lax.all_to_all(cotangent, "fs", split_axis=1, concat_axis=0, tiled=True),
    )
    gate_local = contract_first(columns, lax.all_gather(gate_grad, "fs", axis=0, tiled=True))
    up_local = contract_first(columns, lax.all_gather(up_grad, "fs", axis=0, tiled=True))
    down_local = contract_first(cot_columns, lax.all_gather(hidden_early, "fs", axis=0, tiled=True))
    gate_total, up_total, down_total = (
        lax.psum(gate_local.astype(jnp.bfloat16), "rep").astype(jnp.float32),
        lax.psum(up_local.astype(jnp.bfloat16), "rep").astype(jnp.float32),
        lax.psum(down_local.astype(jnp.bfloat16), "rep").astype(jnp.float32),
    )
    return (
        later_output,
        earlier_input_grad,
        gate_sum + gate_total,
        up_sum + up_total,
        down_sum + down_total,
    )


def solution(mesh):
    placed = (
        P(("rep", "fs"), None),
        P(("rep", "fs"), None),
        P(("rep", "fs"), None),
        P("fs", "tp"),
        P("fs", "tp"),
        P("fs", "tp"),
        P("fs", "tp"),
        P("fs", "tp"),
        P("fs", "tp"),
    )
    reps, shards, blocks = (mesh.shape[axis] for axis in ("rep", "fs", "tp"))

    def chosen(*arrays):
        rows = arrays[0].shape[0]
        depth, units = arrays[3].shape
        layers = shards // 2
        fits = (
            reps == 2
            and blocks == 2
            and layers >= 2
            and shards == 2 * layers
            and layers & (layers - 1) == 0
            and units % (layers * 128) == 0
            and depth % 128 == 0
            and rows % 64 == 0
            and arrays[0].shape[1] % 512 == 0
            and arrays[0].shape[1] == depth * shards
        )
        return split_hidden(shards, *arrays) if fits else per_device(*arrays)

    return jax.shard_map(
        chosen,
        mesh=mesh,
        in_specs=placed,
        out_specs=(
            P(("rep", "fs"), None),
            P(("rep", "fs"), None),
            P("fs", "tp"),
            P("fs", "tp"),
            P("fs", "tp"),
        ),
        check_vma=False,
    )
```

```python
import functools

import jax
import jax.numpy as jnp
from jax import lax
from jax.experimental import pallas as pl
from jax.experimental.pallas import tpu as pltpu
from jax.sharding import PartitionSpec as P

MESH = pl.DeviceIdType.MESH


def flip(index, k, n):
    out, bit = 0, 1
    while bit < n:
        digit = lax.rem(index // bit, 2)
        out = out + bit * ((1 - digit) if k & bit else digit)
        bit *= 2
    return out


def span(start, size, step):
    return pl.ds(pl.multiple_of(start, step), size)


def remote(source, target, send, recv, device):
    return pltpu.make_async_remote_copy(
        src_ref=source,
        dst_ref=target,
        send_sem=send,
        recv_sem=recv,
        device_id=device,
        device_id_type=MESH,
    )


EARLY, COT, LATE = 0, 1, 2


def fused_kernel(
    nz, later, earlier, cot, gw, uw, dw, gsum, usum, dsum, late_out, early_out, gnew, unew, dnew,
    slots, wt, w, g_out, hid, part, peer, rin, rout, gown, gside, gother, gyo, gyi, gxo, gxi, gzo,
    lts, lws, los, lns, wzs, wzr, wxs, wxr, wys, wyr, aos, ags, agr, cs, cr,
    tds, tdr, rss, rsr, os_, or_, gys, gyr, gxs, gxr, gzs, gzr, gfs, gfr,
):
    r, f, t = lax.axis_index("rep"), lax.axis_index("fs"), lax.axis_index("tp")
    y, z = lax.rem(f, 2), f // 2
    m, width = later.shape
    q = m // 2
    dl, u = gw.shape[0], w.shape[2]
    hr, last = dl // 2, nz - 1
    f32, bf16 = jnp.float32, jnp.bfloat16
    outs = (late_out, early_out)
    to_x, to_y, to_t = {"rep": 1 - r}, {"fs": z * 2 + 1 - y}, {"tp": 1 - t}

    def layer(height):
        return {"fs": height * 2 + y}

    def units(height):
        return span(height * u, u, u)

    slot_of = (1, 2, 0)
    local_tokens = [
        pltpu.make_async_copy(source, slots.at[slot_of[g], z], lts.at[g])
        for g, source in enumerate((earlier, cot, later))
    ]
    local_weights = [
        pltpu.make_async_copy(source.at[span(r * hr, hr, hr), :], wt.at[i], lws.at[i])
        for i, source in enumerate((gw, uw, dw))
    ]
    local_own = [
        pltpu.make_async_copy(source.at[:, units(z)], w.at[i, span((z * 2 + y) * dl, dl, dl), :], los.at[i])
        for i, source in enumerate((gw, uw, dw))
    ]
    news = (gnew, unew, dnew)
    local_sums = [pltpu.make_async_copy(source, news[i], lns.at[i]) for i, source in enumerate((gsum, usum, dsum))]
    for copy in local_weights:
        copy.start()

    barrier = pltpu.get_barrier_semaphore()
    for device in [layer(flip(z, k, nz)) for k in range(1, nz)] + [to_x, to_y, to_t]:
        pl.semaphore_signal(barrier, inc=1, device_id=device, device_id_type=MESH)
    pl.semaphore_wait(barrier, nz + 2)

    pending = []

    def go(copy):
        copy.start()
        pending.append((None, copy))

    def when_go(condition, copy):
        @pl.when(condition)
        def _():
            copy.start()

        pending.append((condition, copy))

    def rows(side, height, h):
        return span((height * 2 + side) * dl + h * hr, hr, hr)

    def piece(side, height, h):
        return w.at[:, rows(side, height, h), :]

    def send_weights(height, send, recv, device):
        remote(wt.at[:, :, units(height)], piece(y, z, r), send, recv, device).start()

    def wx(k, a, block):
        return remote(block, block, wxs.at[0], wxr.at[k, a], to_x)

    def wy(k, a, block):
        return remote(block, block, wys.at[0], wyr.at[k, a], to_y)

    def spread(k):
        block = piece(y, flip(z, k, nz), r)
        remote(block, block, wzs.at[0], wzr.at[k], to_x).wait_recv()
        wx(k, 0, block).start()
        wy(k, 0, block).start()

    def relay(k):
        height = flip(z, k, nz)
        if k % 2:
            block = piece(y, height, 1 - r)
            wx(k, 0, block).wait_recv()
            wy(k, 1, block).start()
        else:
            block = piece(1 - y, height, r)
            wy(k, 0, block).wait_recv()
            wx(k, 1, block).start()

    def gathered(k):
        height = flip(z, k, nz)
        if k % 2:
            wy(k, 0, piece(1 - y, height, r)).wait_recv()
            wy(k, 1, piece(1 - y, height, 1 - r)).wait_recv()
        else:
            if k:
                wx(k, 0, piece(y, height, 1 - r)).wait_recv()
            wx(k, 1, piece(1 - y, height, 1 - r)).wait_recv()

    def half(core):
        return span(core * q, q, q)

    def block_of(g, origin, core):
        return slots.at[slot_of[g], origin, half(core), :]

    def step_of(d):
        return 1 - 2 * d

    def exists(height):
        return jnp.logical_and(height >= 0, height < nz)

    def send_own(g, ends=None):
        for d in range(2):
            target = z + step_of(d)
            block = block_of(g, z, t)
            at_end = z == (last if d else 0)
            chosen = exists(target)
            if ends is not None:
                chosen = jnp.logical_and(chosen, at_end if ends else jnp.logical_not(at_end))
            when_go(chosen, remote(block, block, aos.at[g, d], agr.at[g, z], layer(target)))

    def take_on(g, k, ends=None):
        for d in range(2):
            origin, target = z - step_of(d) * k, z + step_of(d)
            block = block_of(g, origin, t)
            ahead = remote(block, block, ags.at[g, max(min(k, last - 1) - 1, 0), d], agr.at[g, origin], layer(target))
            chosen = exists(origin)
            if ends is not None:
                at_end = origin == (last if d else 0)
                chosen = jnp.logical_and(chosen, at_end if ends else jnp.logical_not(at_end))

            @pl.when(chosen)
            def _():
                ahead.wait_recv()

            if k < last:
                when_go(jnp.logical_and(chosen, exists(target)), ahead)

            @pl.when(chosen)
            def _():
                remote(block, block, cs.at[0], cr.at[g, origin], to_t).start()

    def whole(g, k):
        for d in range(2):
            origin = z - step_of(d) * k
            block = block_of(g, origin, 1 - t)

            @pl.when(exists(origin))
            def _():
                remote(block, block, cs.at[0], cr.at[g, origin], to_t).wait_recv()

    def each_block(k, body):
        if k == 0:
            body(z)
            return

        def one(d, carry):
            origin = z - (1 - 2 * d) * k

            @pl.when(exists(origin))
            def _():
                body(origin)

            return carry

        lax.fori_loop(0, 2, one, 0)

    def early(b):
        gate = jnp.dot(slots[1, b], w[0], preferred_element_type=f32)
        up = jnp.dot(slots[1, b], w[1], preferred_element_type=f32)
        hidden_grad = jnp.dot(slots[2, b], w[2], preferred_element_type=f32)
        hid[0, b], hid[1, b], hid[2, b] = early_parts(gate, up, hidden_grad)

    def early_level(k):
        if k:
            whole(EARLY, k)
            whole(COT, k)
        each_block(k, early)

    step = width // 4

    def trade(o, b):
        return remote(part.at[o, b, half(1 - t), :], peer.at[o, b], tds.at[0], tdr.at[o, b], to_t)

    def late(b):
        gate = jnp.dot(slots[0, b], w[0], preferred_element_type=f32)
        up = jnp.dot(slots[0, b], w[1], preferred_element_type=f32)
        hidden = (jax.nn.silu(gate) * up).astype(bf16)
        for c in range(4):
            lanes = slice(c * step, (c + 1) * step)
            part[0, b, :, lanes] = contract_last(hidden, w[2, lanes, :]).astype(bf16)
        trade(0, b).start()

    def late_level(k):
        if k:
            whole(LATE, k)
        each_block(k, late)

    def input_grad(b):
        for c in range(4):
            lanes = slice(c * step, (c + 1) * step)
            part[1, b, :, lanes] = (
                contract_last(hid[0, b], w[0, lanes, :]) + contract_last(hid[1, b], w[1, lanes, :])
            ).astype(bf16)
        trade(1, b).start()

    fine = 16

    def traded(o, b):
        remote(peer.at[o, b], peer.at[o, b], tds.at[0], tdr.at[o, b], to_t).wait_recv()

    def chunks(body):
        def one(i, carry):
            body(i * fine)
            return carry

        lax.fori_loop(0, q // fine, one, 0)

    def own(o, b, start):
        return (
            part[o, b, span(t * q + start, fine, fine), :].astype(f32)
            + peer[o, b, span(start, fine, fine), :].astype(f32)
        )

    def sum_copy(o, d, b, device):
        return remote(rout.at[o, b], rin.at[d, o, b], rss.at[0], rsr.at[d, o, b], device)

    def sum_step(o, far, h):
        @pl.when(jnp.logical_or(z == h, z == nz - 1 - h))
        def _():
            up = jnp.where(z == h, 1, 0)
            d = 1 - up
            b = up * far + d * (nz - 1 - far)
            copy = sum_copy(o, d, b, layer(z + 2 * up - 1))
            traded(o, b)
            if h:
                copy.wait_recv()

            def add(start):
                piece_rows = span(start, fine, fine)
                value = own(o, b, start)
                if h:
                    value = value + rin[d, o, b, piece_rows, :].astype(f32)
                rout[o, b, piece_rows, :] = value.astype(bf16)

            chunks(add)
            copy.start()

    def sum_end(o):
        traded(o, z)
        for d in range(2):
            @pl.when(exists(z - step_of(d)))
            def _():
                sum_copy(o, d, z, to_t).wait_recv()

        def add(start):
            piece_rows = span(start, fine, fine)
            value = own(o, z, start)
            for d in range(2):
                value = value + jnp.where(
                    exists(z - step_of(d)), rin[d, o, z, piece_rows, :].astype(f32), 0.0
                )
            outs[o][span(t * q + start, fine, fine), :] = value.astype(bf16)

        chunks(add)
        mine = outs[o].at[half(t), :]
        go(remote(mine, mine, os_.at[o], or_.at[o], to_t))

    def grad_block(side, height, i):
        lanes = span((height * 2 + side) * dl, dl, dl)
        source = slots[2 if i == 2 else 1, :, :, lanes].reshape(nz * m, dl)
        return contract_first(source, hid[i].reshape(nz * m, u))

    def grad_send(k, i):
        gyo[k, i] = grad_block(1 - y, flip(z, k, nz), i).astype(bf16)
        remote(gyo.at[k, i], gyi.at[k, i], gys.at[0], gyr.at[k, i], to_y).start()

    def grad_own(k, i):
        gown[k, i] = grad_block(y, flip(z, k, nz), i)

    mine_rows, their_rows = span(r * hr, hr, hr), span((1 - r) * hr, hr, hr)

    def grad_x(k, i):
        remote(gyi.at[k, i], gyi.at[k, i], gys.at[0], gyr.at[k, i], to_y).wait_recv()
        gxo[k, i] = (gown[k, i, their_rows, :] + gyi[k, i, their_rows, :].astype(f32)).astype(bf16)
        remote(gxo.at[k, i], gxi.at[k, i], gxs.at[0], gxr.at[k, i], to_x).start()

    def cross_x(k, i):
        return remote(gyo.at[k, i], gyi.at[k, i], gys.at[0], gyr.at[k, i], to_x)

    def cross_y(k, i):
        return remote(gxo.at[k, i], gxi.at[k, i], gxs.at[0], gxr.at[k, i], to_y)

    def cross_send(k, i, c):
        gown[k, i] = grad_block(y, flip(z, k, nz), i)
        gyo[k, i, :hr, :] = gown[k, i, their_rows, :].astype(bf16)
        gside[...] = grad_block(1 - y, flip(z, k, nz), i)
        gyo[k, i, hr:, :] = gside[their_rows, :].astype(bf16)
        gother[c] = gside[mine_rows, :]
        cross_x(k, i).start()

    def cross_turn(k, i, c):
        cross_x(k, i).wait_recv()
        gxo[k, i] = (gother[c] + gyi[k, i, hr:, :].astype(f32)).astype(bf16)
        cross_y(k, i).start()

    def cross_end(k, i, c):
        cross_y(k, i).wait_recv()
        total = (gown[k, i, mine_rows, :] + gyi[k, i, :hr, :].astype(f32) + gxi[k, i].astype(f32)).astype(bf16)
        if k:
            gzo[k, i] = total
            grad_onward(k, i)
        else:
            g_out[i, mine_rows, units(z)] = total
            grad_back(k, i)

    def grad_onward(k, i):
        remote(gzo.at[k, i], g_block(i, z, r), gzs.at[0], gzr.at[k, i], layer(flip(z, k, nz))).start()

    def g_block(i, height, h):
        return g_out.at[i, span(h * hr, hr, hr), units(height)]

    def grad_z(k, i):
        remote(gxi.at[k, i], gxi.at[k, i], gxs.at[0], gxr.at[k, i], to_x).wait_recv()
        total = (
            gown[k, i, mine_rows, :] + gyi[k, i, mine_rows, :].astype(f32) + gxi[k, i].astype(f32)
        ).astype(bf16)
        gzo[k, i] = total
        grad_onward(k, i)

    def g_copy(k, i, h):
        block = g_block(i, flip(z, k, nz), h)
        return remote(block, block, gfs.at[0], gfr.at[k, i], to_x)

    def grad_back(k, i):
        if k:
            block = g_block(i, flip(z, k, nz), r)
            remote(block, block, gzs.at[0], gzr.at[k, i], to_x).wait_recv()
        g_copy(k, i, r).start()
        grad_add(k, i, r)

    def grad_add(k, i, h):
        place = (span(h * hr, hr, hr), units(flip(z, k, nz)))
        news[i][place] += g_out[(i,) + place].astype(f32)

    def grad_last(k, i):
        g_copy(k, i, 1 - r).wait_recv()
        grad_add(k, i, 1 - r)

    def run(name, task, *args):
        with jax.named_scope(name + "_".join(str(a) for a in args if isinstance(a, int))):
            task(*args)

    def send_first():
        for copy in local_weights:
            copy.wait()
        for copy in local_tokens:
            copy.start()
        for k in range(1, nz):
            send_weights(flip(z, k, nz), wzs.at[0], wzr.at[k], layer(flip(z, k, nz)))
        send_weights(z, wys.at[0], wyr.at[0, 0], to_y)
        for copy in local_tokens:
            copy.wait()
        send_own(EARLY)
        send_own(COT)
        send_own(LATE, True)
        for copy in local_own + local_sums:
            copy.start()
        for copy in local_own:
            copy.wait()

    run("send_first", send_first)
    run("relay", relay, 0)
    for k in range(1, nz):
        run("spread", spread, k)
        if k > 1:
            run("relay", relay, k - 1)
    run("take_e", take_on, EARLY, 1)
    run("relay", relay, last)
    run("take_c", take_on, COT, 1)
    for k in range(last):
        run("gathered", gathered, k)
    if last > 1:
        run("take_e", take_on, EARLY, 2)
    run("gathered", gathered, last)
    run("early", early_level, 0)
    if last > 1:
        run("take_c", take_on, COT, 2)
    for k in range(3, last):
        run("take_e", take_on, EARLY, k)
        run("take_c", take_on, COT, k)
    run("send_l", send_own, LATE, False)
    run("take_l_end", take_on, LATE, 1, True)
    for k in range(last - 1, 0, -1):
        run("early", early_level, k)
        if 1 < k + 1 < last:
            run("sum_e", sum_step, 1, k + 1, 0)
        run("input_grad", each_block, k, input_grad)
    if last > 2:
        run("take_e", take_on, EARLY, last)
        run("take_c", take_on, COT, last)
    if last == 1:
        run("early", early_level, 1)
    if last > 1:
        run("early", early_level, last)
    crossing = [(0, 0), (0, 1), (0, 2)] + [(1, i) for i in range(1)]
    order = [(k, i) for k in range(last, 0, -1) for i in range(3) if (k, i) not in crossing]
    def send_next(count):
        for _ in range(count):
            if to_send:
                run("grad_send", grad_send, *to_send.pop(0))

    def wait_sums():
        for copy in local_sums:
            copy.wait()

    def own_next(count):
        for _ in range(count):
            if to_own:
                run("grad_own", grad_own, *to_own.pop(0))

    to_send, to_own = list(order), list(order)
    send_next(1)
    run("cross_send", cross_send, *crossing[0], 0)
    send_next(1)
    run("cross_send", cross_send, *crossing[1], 1)
    run("input_grad", each_block, last, input_grad)
    send_next(2)
    run("take_l", take_on, LATE, 1, False)
    run("sum_e", sum_step, 1, last, 0)
    if last > 1:
        run("sum_e", sum_step, 1, 1, 0)
    run("input_grad", each_block, 0, input_grad)
    send_next(1)
    own_next(2)

    between = {}

    def place(j, *task):
        between.setdefault(j, []).append(task)

    count = len(order)
    for far in range(2, nz):
        for h in range(1, far):
            place(2 * far - 5 + 5 * (h - 1), "sum_e", sum_step, 1, far, h)
    place(-1, "late", late_level, 1)
    if last > 1:
        place(-1, "take_l", take_on, LATE, 2)
    place(-1, "late", late_level, 0)
    for far in range(3, nz):
        place(far - 2, "take_l", take_on, LATE, far)
    for far in range(last, 0, -1):
        if far > 1:
            place(2 * (last - far) + 1, "late", late_level, far)
        place(last - far + 2, "sum_l", sum_step, 0, far, 0)
        for h in range(1, far):
            place(5 + 2 * (last - far) + 5 * (h - 1), "sum_l", sum_step, 0, far, h)
    for c, (k, i) in enumerate(crossing):
        if c > 1:
            place(c, "cross_send", cross_send, k, i, c)
        place((0, 2, 5, 6, 7, 8)[c], "cross_turn", cross_turn, k, i, c)
        place((6, 7, 8, 8, 9, 9)[c], "cross_end", cross_end, k, i, c)
        if k:
            place((6, 7, 8, 8, 9, 9)[c] + 3, "grad_back", grad_back, k, i)
    place(2 * last + 2, "sum_end_e", sum_end, 1)
    for j, (k, i) in enumerate(order):
        place(j + (5 if k > 1 else 4), "grad_back", grad_back, k, i)
    place(12, "sum_end_l", sum_end, 0)
    place(-1, "sums", wait_sums)
    for j in range(min(min(between), -1), max(max(between), count) + 1):
        if 0 <= j < count:
            own_next(1)
            run("grad_x", grad_x, *order[j])
            send_next(1)
        if 1 <= j <= count:
            run("grad_z", grad_z, *order[j - 1])
        for name, task, *args in between.get(j, ()):
            run(name, task, *args)
    for k, i in crossing[:3] + order + crossing[3:]:
        run("grad_last", grad_last, k, i)
    def finish():
        for o in range(2):
            other = outs[o].at[half(1 - t), :]
            remote(other, other, os_.at[o], or_.at[o], to_t).wait_recv()

    def drain():
        def sent(block, sem):
            remote(block, block, sem.at[0], sem.at[0], to_t).wait_send()

        sent(w.at[:, pl.ds(0, last * hr), :], wzs)
        sent(w.at[:, pl.ds(0, (last + nz // 2) * hr), :], wxs)
        sent(w.at[:, pl.ds(0, (nz + nz // 2) * hr), :], wys)
        sent(slots.at[:, pl.ds(0, last), pl.ds(0, q), :], cs)
        sent(peer, tds)
        sent(rout.at[:, pl.ds(0, last)], rss)
        sent(gyo, gys)
        sent(gxo, gxs)
        sent(gzo.at[pl.ds(1, last)], gzs)
        sent(gxo, gfs)
        for condition, copy in pending:
            if condition is None:
                copy.wait_send()
            else:
                @pl.when(condition)
                def _():
                    copy.wait_send()

    run("finish", finish)
    run("drain", drain)


def close_kernel(*refs):
    sems = refs[-1]
    count = (len(refs) - 1) // 2
    copies = [pltpu.make_async_copy(refs[i], refs[count + i], sems.at[i]) for i in range(count)]
    for copy in copies:
        copy.start()
    for copy in copies:
        copy.wait()


def close(*arrays):
    return pl.pallas_call(
        close_kernel,
        out_shape=tuple(jax.ShapeDtypeStruct(a.shape, a.dtype) for a in arrays),
        in_specs=[VMEM] * len(arrays),
        out_specs=(HBM,) * len(arrays),
        scratch_shapes=[dma(len(arrays))],
        compiler_params=pltpu.CompilerParams(vmem_limit_bytes=8 * 2**20),
        name="close",
    )(*arrays)


VMEM = pl.BlockSpec(memory_space=pltpu.VMEM)
HBM = pl.BlockSpec(memory_space=pltpu.HBM)


def dma(*shape):
    return pltpu.SemaphoreType.DMA(shape)


def split_hidden(
    n,
    later_input,
    earlier_input,
    cotangent,
    gate_weight,
    up_weight,
    down_weight,
    gate_sum,
    up_sum,
    down_sum,
):
    bf16, f32 = jnp.bfloat16, jnp.float32
    m, width = later_input.shape
    dl, ff = gate_weight.shape
    nz = n // 2
    u, q, hr = ff // nz, m // 2, dl // 2
    results = pl.pallas_call(
        functools.partial(fused_kernel, nz),
        out_shape=(
            jax.ShapeDtypeStruct((m, width), bf16),
            jax.ShapeDtypeStruct((m, width), bf16),
            jax.ShapeDtypeStruct((dl, ff), f32),
            jax.ShapeDtypeStruct((dl, ff), f32),
            jax.ShapeDtypeStruct((dl, ff), f32),
        ),
        in_specs=[HBM] * 9,
        out_specs=(VMEM,) * 5,
        scratch_shapes=[
            pltpu.VMEM((3, nz, m, width), bf16),
            pltpu.VMEM((3, hr, ff), bf16),
            pltpu.VMEM((3, width, u), bf16),
            pltpu.VMEM((3, dl, ff), bf16),
            pltpu.VMEM((3, nz, m, u), bf16),
            pltpu.VMEM((2, nz, m, width), bf16),
            pltpu.VMEM((2, nz, q, width), bf16),
            pltpu.VMEM((2, 2, nz, q, width), bf16),
            pltpu.VMEM((2, nz, q, width), bf16),
            pltpu.VMEM((nz, 3, dl, u), f32),
            pltpu.VMEM((dl, u), f32),
            pltpu.VMEM((6, hr, u), f32),
            pltpu.VMEM((nz, 3, dl, u), bf16),
            pltpu.VMEM((nz, 3, dl, u), bf16),
            pltpu.VMEM((nz, 3, hr, u), bf16),
            pltpu.VMEM((nz, 3, hr, u), bf16),
            pltpu.VMEM((nz, 3, hr, u), bf16),
        ]
        + [dma(3)] * 4
        + [dma(1), dma(nz), dma(1), dma(nz, 2), dma(1), dma(nz, 2)]
        + [dma(3, 2), dma(3, max(nz - 2, 1), 2), dma(3, nz), dma(1), dma(3, nz)]
        + [dma(1), dma(2, nz), dma(1), dma(2, 2, nz), dma(2), dma(2)]
        + [dma(1), dma(nz, 3)] * 4,
        compiler_params=pltpu.CompilerParams(
            collective_id=0, has_side_effects=True, vmem_limit_bytes=46 * 2**20
        ),
        name="fused",
    )(
        *(
            pltpu.with_memory_space_constraint(a, pltpu.HBM)
            for a in (later_input, earlier_input, cotangent, gate_weight, up_weight, down_weight, gate_sum, up_sum, down_sum)
        )
    )
    return close(*results)


def early_parts(gate_early, up_early, hidden_grad):
    sigmoid_gate = jax.nn.sigmoid(gate_early)
    silu_early = gate_early * sigmoid_gate
    gate_grad = (
        hidden_grad * up_early * sigmoid_gate * (1.0 + gate_early * (1.0 - sigmoid_gate))
    ).astype(jnp.bfloat16)
    up_grad = (hidden_grad * silu_early).astype(jnp.bfloat16)
    hidden_early = (silu_early * up_early).astype(jnp.bfloat16)
    return gate_grad, up_grad, hidden_early


def contract_last(first, second):
    return lax.dot_general(
        first, second, (((1,), (1,)), ((), ())), preferred_element_type=jnp.float32
    )


def contract_first(first, second):
    return lax.dot_general(
        first, second, (((0,), (0,)), ((), ())), preferred_element_type=jnp.float32
    )


def per_device(
    later_input,
    earlier_input,
    cotangent,
    gate_weight,
    up_weight,
    down_weight,
    gate_sum,
    up_sum,
    down_sum,
):
    gate_full, up_full, down_full = (
        lax.all_gather(gate_weight, "fs", axis=0, tiled=True),
        lax.all_gather(up_weight, "fs", axis=0, tiled=True),
        lax.all_gather(down_weight, "fs", axis=0, tiled=True),
    )
    gate_late = jnp.dot(later_input, gate_full, preferred_element_type=jnp.float32)
    up_late = jnp.dot(later_input, up_full, preferred_element_type=jnp.float32)
    hidden_late = (jax.nn.silu(gate_late) * up_late).astype(jnp.bfloat16)
    partial_late = contract_last(hidden_late, down_full)
    later_output = lax.psum(partial_late.astype(jnp.bfloat16), "tp")
    gate_early = jnp.dot(earlier_input, gate_full, preferred_element_type=jnp.float32)
    up_early = jnp.dot(earlier_input, up_full, preferred_element_type=jnp.float32)
    hidden_grad = jnp.dot(cotangent, down_full, preferred_element_type=jnp.float32)
    sigmoid_gate = jax.nn.sigmoid(gate_early)
    silu_early = gate_early * sigmoid_gate
    gate_grad = (
        hidden_grad * up_early * sigmoid_gate * (1.0 + gate_early * (1.0 - sigmoid_gate))
    ).astype(jnp.bfloat16)
    up_grad = (hidden_grad * silu_early).astype(jnp.bfloat16)
    hidden_early = (silu_early * up_early).astype(jnp.bfloat16)
    partial_early = contract_last(gate_grad, gate_full) + contract_last(up_grad, up_full)
    earlier_input_grad = lax.psum(partial_early.astype(jnp.bfloat16), "tp")
    columns, cot_columns = (
        lax.all_to_all(earlier_input, "fs", split_axis=1, concat_axis=0, tiled=True),
        lax.all_to_all(cotangent, "fs", split_axis=1, concat_axis=0, tiled=True),
    )
    gate_local = contract_first(columns, lax.all_gather(gate_grad, "fs", axis=0, tiled=True))
    up_local = contract_first(columns, lax.all_gather(up_grad, "fs", axis=0, tiled=True))
    down_local = contract_first(cot_columns, lax.all_gather(hidden_early, "fs", axis=0, tiled=True))
    gate_total, up_total, down_total = (
        lax.psum(gate_local.astype(jnp.bfloat16), "rep").astype(jnp.float32),
        lax.psum(up_local.astype(jnp.bfloat16), "rep").astype(jnp.float32),
        lax.psum(down_local.astype(jnp.bfloat16), "rep").astype(jnp.float32),
    )
    return (
        later_output,
        earlier_input_grad,
        gate_sum + gate_total,
        up_sum + up_total,
        down_sum + down_total,
    )


def solution(mesh):
    placed = (
        P(("rep", "fs"), None),
        P(("rep", "fs"), None),
        P(("rep", "fs"), None),
        P("fs", "tp"),
        P("fs", "tp"),
        P("fs", "tp"),
        P("fs", "tp"),
        P("fs", "tp"),
        P("fs", "tp"),
    )
    reps, shards, blocks = (mesh.shape[axis] for axis in ("rep", "fs", "tp"))

    def chosen(*arrays):
        rows = arrays[0].shape[0]
        depth, units = arrays[3].shape
        layers = shards // 2
        fits = (
            reps == 2
            and blocks == 2
            and layers >= 2
            and shards == 2 * layers
            and layers & (layers - 1) == 0
            and units % (layers * 128) == 0
            and depth % 128 == 0
            and rows % 64 == 0
            and arrays[0].shape[1] % 512 == 0
            and arrays[0].shape[1] == depth * shards
        )
        return split_hidden(shards, *arrays) if fits else per_device(*arrays)

    return jax.shard_map(
        chosen,
        mesh=mesh,
        in_specs=placed,
        out_specs=(
            P(("rep", "fs"), None),
            P(("rep", "fs"), None),
            P("fs", "tp"),
            P("fs", "tp"),
            P("fs", "tp"),
        ),
        check_vma=False,
    )
```

```python
import functools

import jax
import jax.numpy as jnp
from jax import lax
from jax.experimental import pallas as pl
from jax.experimental.pallas import tpu as pltpu
from jax.sharding import PartitionSpec as P

MESH = pl.DeviceIdType.MESH


def flip(index, k, n):
    out, bit = 0, 1
    while bit < n:
        digit = lax.rem(index // bit, 2)
        out = out + bit * ((1 - digit) if k & bit else digit)
        bit *= 2
    return out


def span(start, size, step):
    return pl.ds(pl.multiple_of(start, step), size)


def remote(source, target, send, recv, device):
    return pltpu.make_async_remote_copy(
        src_ref=source,
        dst_ref=target,
        send_sem=send,
        recv_sem=recv,
        device_id=device,
        device_id_type=MESH,
    )


EARLY, COT, LATE = 0, 1, 2


def fused_kernel(
    nz, later, earlier, cot, gw, uw, dw, gsum, usum, dsum, late_out, early_out, gnew, unew, dnew,
    slots, wt, w, g_out, hid, part, peer, rin, rout, gown, gside, gother, gyo, gyi, gxo, gxi, gzo,
    lts, lws, los, lns, wzs, wzr, wxs, wxr, wys, wyr, aos, ags, agr, cs, cr,
    tds, tdr, rss, rsr, os_, or_, gys, gyr, gxs, gxr, gzs, gzr, gfs, gfr,
):
    r, f, t = lax.axis_index("rep"), lax.axis_index("fs"), lax.axis_index("tp")
    y, z = lax.rem(f, 2), f // 2
    m, width = later.shape
    q = m // 2
    dl, u = gw.shape[0], w.shape[2]
    hr, last = dl // 2, nz - 1
    f32, bf16 = jnp.float32, jnp.bfloat16
    outs = (late_out, early_out)
    to_x, to_y, to_t = {"rep": 1 - r}, {"fs": z * 2 + 1 - y}, {"tp": 1 - t}

    def layer(height):
        return {"fs": height * 2 + y}

    def units(height):
        return span(height * u, u, u)

    slot_of = (1, 2, 0)
    local_tokens = [
        pltpu.make_async_copy(source, slots.at[slot_of[g], z], lts.at[g])
        for g, source in enumerate((earlier, cot, later))
    ]
    local_weights = [
        pltpu.make_async_copy(source.at[span(r * hr, hr, hr), :], wt.at[i], lws.at[i])
        for i, source in enumerate((gw, uw, dw))
    ]
    local_own = [
        pltpu.make_async_copy(source.at[:, units(z)], w.at[i, span((z * 2 + y) * dl, dl, dl), :], los.at[i])
        for i, source in enumerate((gw, uw, dw))
    ]
    news = (gnew, unew, dnew)
    local_sums = [pltpu.make_async_copy(source, news[i], lns.at[i]) for i, source in enumerate((gsum, usum, dsum))]
    for copy in local_weights:
        copy.start()

    barrier = pltpu.get_barrier_semaphore()
    for device in [layer(flip(z, k, nz)) for k in range(1, nz)] + [to_x, to_y, to_t]:
        pl.semaphore_signal(barrier, inc=1, device_id=device, device_id_type=MESH)
    pl.semaphore_wait(barrier, nz + 2)

    pending = []

    def go(copy):
        copy.start()
        pending.append((None, copy))

    def when_go(condition, copy):
        @pl.when(condition)
        def _():
            copy.start()

        pending.append((condition, copy))

    def rows(side, height, h):
        return span((height * 2 + side) * dl + h * hr, hr, hr)

    def piece(side, height, h):
        return w.at[:, rows(side, height, h), :]

    def send_weights(height, send, recv, device):
        remote(wt.at[:, :, units(height)], piece(y, z, r), send, recv, device).start()

    def wx(k, a, block):
        return remote(block, block, wxs.at[0], wxr.at[k, a], to_x)

    def wy(k, a, block):
        return remote(block, block, wys.at[0], wyr.at[k, a], to_y)

    def spread(k):
        block = piece(y, flip(z, k, nz), r)
        remote(block, block, wzs.at[0], wzr.at[k], to_x).wait_recv()
        wx(k, 0, block).start()
        wy(k, 0, block).start()

    def relay(k):
        height = flip(z, k, nz)
        if k % 2:
            block = piece(y, height, 1 - r)
            wx(k, 0, block).wait_recv()
            wy(k, 1, block).start()
        else:
            block = piece(1 - y, height, r)
            wy(k, 0, block).wait_recv()
            wx(k, 1, block).start()

    def gathered(k):
        height = flip(z, k, nz)
        if k % 2:
            wy(k, 0, piece(1 - y, height, r)).wait_recv()
            wy(k, 1, piece(1 - y, height, 1 - r)).wait_recv()
        else:
            if k:
                wx(k, 0, piece(y, height, 1 - r)).wait_recv()
            wx(k, 1, piece(1 - y, height, 1 - r)).wait_recv()

    def half(core):
        return span(core * q, q, q)

    def block_of(g, origin, core):
        return slots.at[slot_of[g], origin, half(core), :]

    def step_of(d):
        return 1 - 2 * d

    def exists(height):
        return jnp.logical_and(height >= 0, height < nz)

    def send_own(g, ends=None):
        for d in range(2):
            target = z + step_of(d)
            block = block_of(g, z, t)
            at_end = z == (last if d else 0)
            chosen = exists(target)
            if ends is not None:
                chosen = jnp.logical_and(chosen, at_end if ends else jnp.logical_not(at_end))
            when_go(chosen, remote(block, block, aos.at[g, d], agr.at[g, z], layer(target)))

    def take_on(g, k, ends=None):
        for d in range(2):
            origin, target = z - step_of(d) * k, z + step_of(d)
            block = block_of(g, origin, t)
            ahead = remote(block, block, ags.at[g, max(min(k, last - 1) - 1, 0), d], agr.at[g, origin], layer(target))
            chosen = exists(origin)
            if ends is not None:
                at_end = origin == (last if d else 0)
                chosen = jnp.logical_and(chosen, at_end if ends else jnp.logical_not(at_end))

            @pl.when(chosen)
            def _():
                ahead.wait_recv()

            if k < last:
                when_go(jnp.logical_and(chosen, exists(target)), ahead)

            @pl.when(chosen)
            def _():
                remote(block, block, cs.at[0], cr.at[g, origin], to_t).start()

    def whole(g, k):
        for d in range(2):
            origin = z - step_of(d) * k
            block = block_of(g, origin, 1 - t)

            @pl.when(exists(origin))
            def _():
                remote(block, block, cs.at[0], cr.at[g, origin], to_t).wait_recv()

    def each_block(k, body):
        if k == 0:
            body(z)
            return

        def one(d, carry):
            origin = z - (1 - 2 * d) * k

            @pl.when(exists(origin))
            def _():
                body(origin)

            return carry

        lax.fori_loop(0, 2, one, 0)

    def early(b):
        gate = jnp.dot(slots[1, b], w[0], preferred_element_type=f32)
        up = jnp.dot(slots[1, b], w[1], preferred_element_type=f32)
        hidden_grad = jnp.dot(slots[2, b], w[2], preferred_element_type=f32)
        hid[0, b], hid[1, b], hid[2, b] = early_parts(gate, up, hidden_grad)

    def early_level(k):
        if k:
            whole(EARLY, k)
            whole(COT, k)
        each_block(k, early)

    step = width // 4

    def trade(o, b):
        return remote(part.at[o, b, half(1 - t), :], peer.at[o, b], tds.at[0], tdr.at[o, b], to_t)

    def late(b):
        gate = jnp.dot(slots[0, b], w[0], preferred_element_type=f32)
        up = jnp.dot(slots[0, b], w[1], preferred_element_type=f32)
        hidden = (jax.nn.silu(gate) * up).astype(bf16)
        for c in range(4):
            lanes = slice(c * step, (c + 1) * step)
            part[0, b, :, lanes] = contract_last(hidden, w[2, lanes, :]).astype(bf16)
        trade(0, b).start()

    def late_level(k):
        if k:
            whole(LATE, k)
        each_block(k, late)

    def input_grad(b):
        for c in range(4):
            lanes = slice(c * step, (c + 1) * step)
            part[1, b, :, lanes] = (
                contract_last(hid[0, b], w[0, lanes, :]) + contract_last(hid[1, b], w[1, lanes, :])
            ).astype(bf16)
        trade(1, b).start()

    fine = 16

    def traded(o, b):
        remote(peer.at[o, b], peer.at[o, b], tds.at[0], tdr.at[o, b], to_t).wait_recv()

    def chunks(body):
        def one(i, carry):
            body(i * fine)
            return carry

        lax.fori_loop(0, q // fine, one, 0)

    def own(o, b, start):
        return (
            part[o, b, span(t * q + start, fine, fine), :].astype(f32)
            + peer[o, b, span(start, fine, fine), :].astype(f32)
        )

    def sum_copy(o, d, b, device):
        return remote(rout.at[o, b], rin.at[d, o, b], rss.at[0], rsr.at[d, o, b], device)

    def sum_step(o, far, h):
        @pl.when(jnp.logical_or(z == h, z == nz - 1 - h))
        def _():
            up = jnp.where(z == h, 1, 0)
            d = 1 - up
            b = up * far + d * (nz - 1 - far)
            copy = sum_copy(o, d, b, layer(z + 2 * up - 1))
            traded(o, b)
            if h:
                copy.wait_recv()

            def add(start):
                piece_rows = span(start, fine, fine)
                value = own(o, b, start)
                if h:
                    value = value + rin[d, o, b, piece_rows, :].astype(f32)
                rout[o, b, piece_rows, :] = value.astype(bf16)

            chunks(add)
            copy.start()

    def sum_end(o):
        traded(o, z)
        for d in range(2):
            @pl.when(exists(z - step_of(d)))
            def _():
                sum_copy(o, d, z, to_t).wait_recv()

        def add(start):
            piece_rows = span(start, fine, fine)
            value = own(o, z, start)
            for d in range(2):
                value = value + jnp.where(
                    exists(z - step_of(d)), rin[d, o, z, piece_rows, :].astype(f32), 0.0
                )
            outs[o][span(t * q + start, fine, fine), :] = value.astype(bf16)

        chunks(add)
        mine = outs[o].at[half(t), :]
        go(remote(mine, mine, os_.at[o], or_.at[o], to_t))

    def grad_block(side, height, i):
        lanes = span((height * 2 + side) * dl, dl, dl)
        source = slots[2 if i == 2 else 1, :, :, lanes].reshape(nz * m, dl)
        return contract_first(source, hid[i].reshape(nz * m, u))

    def grad_send(k, i):
        gyo[k, i] = grad_block(1 - y, flip(z, k, nz), i).astype(bf16)
        remote(gyo.at[k, i], gyi.at[k, i], gys.at[0], gyr.at[k, i], to_y).start()

    def grad_own(k, i):
        gown[k, i] = grad_block(y, flip(z, k, nz), i)

    mine_rows, their_rows = span(r * hr, hr, hr), span((1 - r) * hr, hr, hr)

    def grad_x(k, i):
        remote(gyi.at[k, i], gyi.at[k, i], gys.at[0], gyr.at[k, i], to_y).wait_recv()
        gxo[k, i] = (gown[k, i, their_rows, :] + gyi[k, i, their_rows, :].astype(f32)).astype(bf16)
        remote(gxo.at[k, i], gxi.at[k, i], gxs.at[0], gxr.at[k, i], to_x).start()

    def cross_x(k, i):
        return remote(gyo.at[k, i], gyi.at[k, i], gys.at[0], gyr.at[k, i], to_x)

    def cross_y(k, i):
        return remote(gxo.at[k, i], gxi.at[k, i], gxs.at[0], gxr.at[k, i], to_y)

    def cross_send(k, i, c):
        gown[k, i] = grad_block(y, flip(z, k, nz), i)
        gyo[k, i, :hr, :] = gown[k, i, their_rows, :].astype(bf16)
        gside[...] = grad_block(1 - y, flip(z, k, nz), i)
        gyo[k, i, hr:, :] = gside[their_rows, :].astype(bf16)
        gother[c] = gside[mine_rows, :]
        cross_x(k, i).start()

    def cross_turn(k, i, c):
        cross_x(k, i).wait_recv()
        gxo[k, i] = (gother[c] + gyi[k, i, hr:, :].astype(f32)).astype(bf16)
        cross_y(k, i).start()

    def cross_end(k, i, c):
        cross_y(k, i).wait_recv()
        total = (gown[k, i, mine_rows, :] + gyi[k, i, :hr, :].astype(f32) + gxi[k, i].astype(f32)).astype(bf16)
        if k:
            gzo[k, i] = total
            grad_onward(k, i)
        else:
            g_out[i, mine_rows, units(z)] = total
            grad_back(k, i)

    def grad_onward(k, i):
        remote(gzo.at[k, i], g_block(i, z, r), gzs.at[0], gzr.at[k, i], layer(flip(z, k, nz))).start()

    def g_block(i, height, h):
        return g_out.at[i, span(h * hr, hr, hr), units(height)]

    def grad_z(k, i):
        remote(gxi.at[k, i], gxi.at[k, i], gxs.at[0], gxr.at[k, i], to_x).wait_recv()
        total = (
            gown[k, i, mine_rows, :] + gyi[k, i, mine_rows, :].astype(f32) + gxi[k, i].astype(f32)
        ).astype(bf16)
        gzo[k, i] = total
        grad_onward(k, i)

    def g_copy(k, i, h):
        block = g_block(i, flip(z, k, nz), h)
        return remote(block, block, gfs.at[0], gfr.at[k, i], to_x)

    def grad_back(k, i):
        if k:
            block = g_block(i, flip(z, k, nz), r)
            remote(block, block, gzs.at[0], gzr.at[k, i], to_x).wait_recv()
        g_copy(k, i, r).start()
        grad_add(k, i, r)

    def grad_add(k, i, h):
        place = (span(h * hr, hr, hr), units(flip(z, k, nz)))
        news[i][place] += g_out[(i,) + place].astype(f32)

    def grad_last(k, i):
        g_copy(k, i, 1 - r).wait_recv()
        grad_add(k, i, 1 - r)

    def run(name, task, *args):
        with jax.named_scope(name + "_".join(str(a) for a in args if isinstance(a, int))):
            task(*args)

    def send_first():
        for copy in local_weights:
            copy.wait()
        for copy in local_tokens:
            copy.start()
        for k in range(1, nz):
            send_weights(flip(z, k, nz), wzs.at[0], wzr.at[k], layer(flip(z, k, nz)))
        send_weights(z, wys.at[0], wyr.at[0, 0], to_y)
        for copy in local_tokens:
            copy.wait()
        send_own(EARLY)
        send_own(COT)
        send_own(LATE, True)
        for copy in local_own + local_sums:
            copy.start()
        for copy in local_own:
            copy.wait()

    run("send_first", send_first)
    run("relay", relay, 0)
    for k in range(1, nz):
        run("spread", spread, k)
        if k > 1:
            run("relay", relay, k - 1)
    run("take_e", take_on, EARLY, 1)
    run("relay", relay, last)
    run("take_c", take_on, COT, 1)
    for k in range(last):
        run("gathered", gathered, k)
    if last > 1:
        run("take_e", take_on, EARLY, 2)
    run("gathered", gathered, last)
    run("early", early_level, 0)
    if last > 1:
        run("take_c", take_on, COT, 2)
    for k in range(3, last):
        run("take_e", take_on, EARLY, k)
        run("take_c", take_on, COT, k)
    run("send_l", send_own, LATE, False)
    run("take_l_end", take_on, LATE, 1, True)
    for k in range(last - 1, 0, -1):
        run("early", early_level, k)
        if 1 < k + 1 < last:
            run("sum_e", sum_step, 1, k + 1, 0)
        run("input_grad", each_block, k, input_grad)
    if last > 2:
        run("take_e", take_on, EARLY, last)
        run("take_c", take_on, COT, last)
    if last == 1:
        run("early", early_level, 1)
    if last > 1:
        run("early", early_level, last)
    crossing = [(0, 0), (0, 1), (0, 2)] + [(1, i) for i in range(1)]
    order = [(k, i) for k in range(last, 0, -1) for i in range(3) if (k, i) not in crossing]
    def send_next(count):
        for _ in range(count):
            if to_send:
                run("grad_send", grad_send, *to_send.pop(0))

    def wait_sums():
        for copy in local_sums:
            copy.wait()

    def own_next(count):
        for _ in range(count):
            if to_own:
                run("grad_own", grad_own, *to_own.pop(0))

    to_send, to_own = list(order), list(order)
    send_next(1)
    run("cross_send", cross_send, *crossing[0], 0)
    send_next(1)
    run("cross_send", cross_send, *crossing[1], 1)
    run("input_grad", each_block, last, input_grad)
    send_next(2)
    run("take_l", take_on, LATE, 1, False)
    run("sum_e", sum_step, 1, last, 0)
    if last > 1:
        run("sum_e", sum_step, 1, 1, 0)
    run("input_grad", each_block, 0, input_grad)
    send_next(1)
    own_next(2)

    between = {}

    def place(j, *task):
        between.setdefault(j, []).append(task)

    count = len(order)
    for far in range(2, nz):
        for h in range(1, far):
            place(2 * far - 5 + 5 * (h - 1), "sum_e", sum_step, 1, far, h)
    place(-1, "late", late_level, 1)
    if last > 1:
        place(-1, "take_l", take_on, LATE, 2)
    place(-1, "late", late_level, 0)
    for far in range(3, nz):
        place(far - 2, "take_l", take_on, LATE, far)
    for far in range(last, 0, -1):
        if far > 1:
            place(2 * (last - far) + 1, "late", late_level, far)
        place(last - far + 2, "sum_l", sum_step, 0, far, 0)
        for h in range(1, far):
            place(5 + 2 * (last - far) + 5 * (h - 1), "sum_l", sum_step, 0, far, h)
    for c, (k, i) in enumerate(crossing):
        if c > 1:
            place(c - 2, "cross_send", cross_send, k, i, c)
        place((0, 2, 4, 5, 7, 8)[c], "cross_turn", cross_turn, k, i, c)
        place((6, 7, 8, 8, 9, 9)[c], "cross_end", cross_end, k, i, c)
        if k:
            place((6, 7, 8, 8, 9, 9)[c] + 3, "grad_back", grad_back, k, i)
    place(2 * last + 2, "sum_end_e", sum_end, 1)
    for j, (k, i) in enumerate(order):
        place(j + (5 if k > 1 else 4), "grad_back", grad_back, k, i)
    place(12, "sum_end_l", sum_end, 0)
    place(-1, "sums", wait_sums)
    for j in range(min(min(between), -1), max(max(between), count) + 1):
        if 0 <= j < count:
            own_next(1)
            run("grad_x", grad_x, *order[j])
            send_next(1)
        if 1 <= j <= count:
            run("grad_z", grad_z, *order[j - 1])
        for name, task, *args in between.get(j, ()):
            run(name, task, *args)
    for k, i in crossing[:3] + order + crossing[3:]:
        run("grad_last", grad_last, k, i)
    def finish():
        for o in range(2):
            other = outs[o].at[half(1 - t), :]
            remote(other, other, os_.at[o], or_.at[o], to_t).wait_recv()

    def drain():
        def sent(block, sem):
            remote(block, block, sem.at[0], sem.at[0], to_t).wait_send()

        sent(w.at[:, pl.ds(0, last * hr), :], wzs)
        sent(w.at[:, pl.ds(0, (last + nz // 2) * hr), :], wxs)
        sent(w.at[:, pl.ds(0, (nz + nz // 2) * hr), :], wys)
        sent(slots.at[:, pl.ds(0, last), pl.ds(0, q), :], cs)
        sent(peer, tds)
        sent(rout.at[:, pl.ds(0, last)], rss)
        sent(gyo, gys)
        sent(gxo, gxs)
        sent(gzo.at[pl.ds(1, last)], gzs)
        sent(gxo, gfs)
        for condition, copy in pending:
            if condition is None:
                copy.wait_send()
            else:
                @pl.when(condition)
                def _():
                    copy.wait_send()

    run("finish", finish)
    run("drain", drain)


def close_kernel(*refs):
    sems = refs[-1]
    count = (len(refs) - 1) // 2
    copies = [pltpu.make_async_copy(refs[i], refs[count + i], sems.at[i]) for i in range(count)]
    for copy in copies:
        copy.start()
    for copy in copies:
        copy.wait()


def close(*arrays):
    return pl.pallas_call(
        close_kernel,
        out_shape=tuple(jax.ShapeDtypeStruct(a.shape, a.dtype) for a in arrays),
        in_specs=[VMEM] * len(arrays),
        out_specs=(HBM,) * len(arrays),
        scratch_shapes=[dma(len(arrays))],
        compiler_params=pltpu.CompilerParams(vmem_limit_bytes=8 * 2**20),
        name="close",
    )(*arrays)


VMEM = pl.BlockSpec(memory_space=pltpu.VMEM)
HBM = pl.BlockSpec(memory_space=pltpu.HBM)


def dma(*shape):
    return pltpu.SemaphoreType.DMA(shape)


def split_hidden(
    n,
    later_input,
    earlier_input,
    cotangent,
    gate_weight,
    up_weight,
    down_weight,
    gate_sum,
    up_sum,
    down_sum,
):
    bf16, f32 = jnp.bfloat16, jnp.float32
    m, width = later_input.shape
    dl, ff = gate_weight.shape
    nz = n // 2
    u, q, hr = ff // nz, m // 2, dl // 2
    results = pl.pallas_call(
        functools.partial(fused_kernel, nz),
        out_shape=(
            jax.ShapeDtypeStruct((m, width), bf16),
            jax.ShapeDtypeStruct((m, width), bf16),
            jax.ShapeDtypeStruct((dl, ff), f32),
            jax.ShapeDtypeStruct((dl, ff), f32),
            jax.ShapeDtypeStruct((dl, ff), f32),
        ),
        in_specs=[HBM] * 9,
        out_specs=(VMEM,) * 5,
        scratch_shapes=[
            pltpu.VMEM((3, nz, m, width), bf16),
            pltpu.VMEM((3, hr, ff), bf16),
            pltpu.VMEM((3, width, u), bf16),
            pltpu.VMEM((3, dl, ff), bf16),
            pltpu.VMEM((3, nz, m, u), bf16),
            pltpu.VMEM((2, nz, m, width), bf16),
            pltpu.VMEM((2, nz, q, width), bf16),
            pltpu.VMEM((2, 2, nz, q, width), bf16),
            pltpu.VMEM((2, nz, q, width), bf16),
            pltpu.VMEM((nz, 3, dl, u), f32),
            pltpu.VMEM((dl, u), f32),
            pltpu.VMEM((6, hr, u), f32),
            pltpu.VMEM((nz, 3, dl, u), bf16),
            pltpu.VMEM((nz, 3, dl, u), bf16),
            pltpu.VMEM((nz, 3, hr, u), bf16),
            pltpu.VMEM((nz, 3, hr, u), bf16),
            pltpu.VMEM((nz, 3, hr, u), bf16),
        ]
        + [dma(3)] * 4
        + [dma(1), dma(nz), dma(1), dma(nz, 2), dma(1), dma(nz, 2)]
        + [dma(3, 2), dma(3, max(nz - 2, 1), 2), dma(3, nz), dma(1), dma(3, nz)]
        + [dma(1), dma(2, nz), dma(1), dma(2, 2, nz), dma(2), dma(2)]
        + [dma(1), dma(nz, 3)] * 4,
        compiler_params=pltpu.CompilerParams(
            collective_id=0, has_side_effects=True, vmem_limit_bytes=46 * 2**20
        ),
        name="fused",
    )(
        *(
            pltpu.with_memory_space_constraint(a, pltpu.HBM)
            for a in (later_input, earlier_input, cotangent, gate_weight, up_weight, down_weight, gate_sum, up_sum, down_sum)
        )
    )
    return close(*results)


def early_parts(gate_early, up_early, hidden_grad):
    sigmoid_gate = jax.nn.sigmoid(gate_early)
    silu_early = gate_early * sigmoid_gate
    gate_grad = (
        hidden_grad * up_early * sigmoid_gate * (1.0 + gate_early * (1.0 - sigmoid_gate))
    ).astype(jnp.bfloat16)
    up_grad = (hidden_grad * silu_early).astype(jnp.bfloat16)
    hidden_early = (silu_early * up_early).astype(jnp.bfloat16)
    return gate_grad, up_grad, hidden_early


def contract_last(first, second):
    return lax.dot_general(
        first, second, (((1,), (1,)), ((), ())), preferred_element_type=jnp.float32
    )


def contract_first(first, second):
    return lax.dot_general(
        first, second, (((0,), (0,)), ((), ())), preferred_element_type=jnp.float32
    )


def per_device(
    later_input,
    earlier_input,
    cotangent,
    gate_weight,
    up_weight,
    down_weight,
    gate_sum,
    up_sum,
    down_sum,
):
    gate_full, up_full, down_full = (
        lax.all_gather(gate_weight, "fs", axis=0, tiled=True),
        lax.all_gather(up_weight, "fs", axis=0, tiled=True),
        lax.all_gather(down_weight, "fs", axis=0, tiled=True),
    )
    gate_late = jnp.dot(later_input, gate_full, preferred_element_type=jnp.float32)
    up_late = jnp.dot(later_input, up_full, preferred_element_type=jnp.float32)
    hidden_late = (jax.nn.silu(gate_late) * up_late).astype(jnp.bfloat16)
    partial_late = contract_last(hidden_late, down_full)
    later_output = lax.psum(partial_late.astype(jnp.bfloat16), "tp")
    gate_early = jnp.dot(earlier_input, gate_full, preferred_element_type=jnp.float32)
    up_early = jnp.dot(earlier_input, up_full, preferred_element_type=jnp.float32)
    hidden_grad = jnp.dot(cotangent, down_full, preferred_element_type=jnp.float32)
    sigmoid_gate = jax.nn.sigmoid(gate_early)
    silu_early = gate_early * sigmoid_gate
    gate_grad = (
        hidden_grad * up_early * sigmoid_gate * (1.0 + gate_early * (1.0 - sigmoid_gate))
    ).astype(jnp.bfloat16)
    up_grad = (hidden_grad * silu_early).astype(jnp.bfloat16)
    hidden_early = (silu_early * up_early).astype(jnp.bfloat16)
    partial_early = contract_last(gate_grad, gate_full) + contract_last(up_grad, up_full)
    earlier_input_grad = lax.psum(partial_early.astype(jnp.bfloat16), "tp")
    columns, cot_columns = (
        lax.all_to_all(earlier_input, "fs", split_axis=1, concat_axis=0, tiled=True),
        lax.all_to_all(cotangent, "fs", split_axis=1, concat_axis=0, tiled=True),
    )
    gate_local = contract_first(columns, lax.all_gather(gate_grad, "fs", axis=0, tiled=True))
    up_local = contract_first(columns, lax.all_gather(up_grad, "fs", axis=0, tiled=True))
    down_local = contract_first(cot_columns, lax.all_gather(hidden_early, "fs", axis=0, tiled=True))
    gate_total, up_total, down_total = (
        lax.psum(gate_local.astype(jnp.bfloat16), "rep").astype(jnp.float32),
        lax.psum(up_local.astype(jnp.bfloat16), "rep").astype(jnp.float32),
        lax.psum(down_local.astype(jnp.bfloat16), "rep").astype(jnp.float32),
    )
    return (
        later_output,
        earlier_input_grad,
        gate_sum + gate_total,
        up_sum + up_total,
        down_sum + down_total,
    )


def solution(mesh):
    placed = (
        P(("rep", "fs"), None),
        P(("rep", "fs"), None),
        P(("rep", "fs"), None),
        P("fs", "tp"),
        P("fs", "tp"),
        P("fs", "tp"),
        P("fs", "tp"),
        P("fs", "tp"),
        P("fs", "tp"),
    )
    reps, shards, blocks = (mesh.shape[axis] for axis in ("rep", "fs", "tp"))

    def chosen(*arrays):
        rows = arrays[0].shape[0]
        depth, units = arrays[3].shape
        layers = shards // 2
        fits = (
            reps == 2
            and blocks == 2
            and layers >= 2
            and shards == 2 * layers
            and layers & (layers - 1) == 0
            and units % (layers * 128) == 0
            and depth % 128 == 0
            and rows % 64 == 0
            and arrays[0].shape[1] % 512 == 0
            and arrays[0].shape[1] == depth * shards
        )
        return split_hidden(shards, *arrays) if fits else per_device(*arrays)

    return jax.shard_map(
        chosen,
        mesh=mesh,
        in_specs=placed,
        out_specs=(
            P(("rep", "fs"), None),
            P(("rep", "fs"), None),
            P("fs", "tp"),
            P("fs", "tp"),
            P("fs", "tp"),
        ),
        check_vma=False,
    )
```
